256 devices in a mesh: ep: 64 (over z, y, core), tp: 4 (over x).
Axes of the slice: x: 4, y: 4, z: 8, core: 2. Of those that a mesh axis runs over, the one named last changes fastest.
Arguments:
- queries: bfloat16 [12288, 8, 128], P('ep', 'tp'), may hold values from -140 to 140
- keys: bfloat16 [12288, 4, 128], P('ep', 'tp'), may hold values from -6 to 6
- values: bfloat16 [12288, 4, 128], P('ep', 'tp'), may hold values from -6 to 6
- mix_scale: float32 [8], P('tp'), may hold values from 0.3 to 0.8
- head_gain: float32 [128], replicated, may hold values from 0.1 to 1.9
- out_weight: bfloat16 [8, 128, 2048], P('tp'), may hold values from -0.1875 to 0.1875
- moe_input: bfloat16 [24576, 2048], P(('ep', 'tp')), may hold values from -6 to 6
- norm_gain: float32 [2048], replicated, may hold values from 0.1 to 1.9
- routes: int32 [24576, 2], P(('ep', 'tp')), may hold values from 0 to 63, all different within a row; in each aligned block of 96 rows (0 to 95, 96 to 191, ...) at most 4 rows name the same one
- route_weights: float32 [24576, 2], P(('ep', 'tp')), may hold values from 0.2 to 1
- gate_weight: bfloat16 [64, 2048, 3584], P('ep', None, 'tp'), may hold values from -0.125 to 0.125
- up_weight: bfloat16 [64, 2048, 3584], P('ep', None, 'tp'), may hold values from -0.125 to 0.125
- down_weight: bfloat16 [64, 3584, 2048], P('ep', 'tp'), may hold values from -0.09375 to 0.09375
Outputs:
- attn_out: bfloat16 [12288, 2048], P(('ep', 'tp'))
- moe_out: bfloat16 [24576, 2048], P(('ep', 'tp'))
The draws below stay inside these ranges and needn't reach their ends.
Inputs may be any that keep to these rules, and one draw needn't show every extreme that they name: `routes`: the 2 experts of a row differ. In each aligned block of 96 rows (the rows of one device) no expert is named by more than 4 rows, and in some blocks an expert is named by exactly 4 rows.
All inputs are finite; a program needn't handle non-finite values.
Results may differ from the reference program's by a relative error of at most 0.014.
Values may be sent and summed in bfloat16 or wider, within the bound.
A program may use at most 128 MiB of HBM per device.

```python
import math
import jax
import jax.numpy as jnp
import numpy as np
from jax import lax

D = 2048
HEADS = 8
KV_HEADS = 4
HD = 64
VD = 128
FFE = 3584
TOPK = 2
TA = 192
TOK_M = 96
SEQ = 12288
TOKENS_M = 24576
EXPERTS = 64
CAP = 4
N_EP = 64
N_TP = 4


def plant_rows(key):
    base = jax.random.fold_in(key, 11)
    query_key, key_key = jax.random.split(base, 2)
    query_draw = 1.3 * jax.random.truncated_normal(query_key, -4.0, 4.0, (SEQ, HEADS, 2, HD), jnp.float32)
    key_draw = 1.3 * jax.random.truncated_normal(key_key, -4.0, 4.0, (SEQ, KV_HEADS, 2, HD), jnp.float32)
    return (query_draw.reshape(SEQ, HEADS, 2 * HD), key_draw.reshape(SEQ, KV_HEADS, 2 * HD))


def draw_queries(key, part):
    return plant_rows(key)[0].astype(jnp.bfloat16)


def draw_keys(key, part):
    return plant_rows(key)[1].astype(jnp.bfloat16)


def steps_of(rng, dims, cuts, smallest, high):
    level, own = 1.0, jax.random.fold_in(rng, 6)
    for position, shards_of in cuts:
        heights = jnp.exp(jax.random.uniform(jax.random.fold_in(own, position), (shards_of,), jnp.float32, smallest / len(cuts), high / len(cuts)))
        level = level * jnp.repeat(heights, dims[position] // shards_of).reshape([-1 if axis == position else 1 for axis in range(len(dims))])
    return level


def deal_out(stream_key, own, number, rows, count, top, most, lean):
    sequence = jax.random.permutation(stream_key, count)
    packed, common = portions_of(count, rows * top, most, lean, True), portions_of(count, rows * top, most, lean, False)
    places = jnp.arange(count)

    def named(sizes, turn):
        used = int((sizes > 0).sum())
        fixed = max(1, used // 4)
        shifted = fixed + (places - fixed + turn * (used - fixed)) % max(1, count - fixed)
        return jnp.zeros((count,), jnp.int32).at[sequence[jnp.where(places < fixed, places, shifted)]].set(jnp.asarray(sizes, jnp.int32))

    sizes = jnp.where(number % 4 == 0, named(packed, number // 4), named(common, number - number // 4 - 1))
    mixed = jax.random.permutation(jax.random.fold_in(own, 3), count)
    source_of, taker = mixed[0:count // 2 * 2:2], mixed[1:count // 2 * 2:2]
    margin = jnp.minimum(sizes[source_of] - 1, most - sizes[taker]) // 2
    margin = jnp.where((source_of == sequence[0]) | (taker == sequence[0]) | (sizes[taker] == 0), 0, jnp.maximum(margin, 0))
    shifted = jax.random.randint(jax.random.fold_in(own, 4), (count // 2,), 0, 1 << 20) % (margin + 1)
    sizes = sizes.at[source_of].add(-shifted).at[taker].add(shifted)
    items = jnp.searchsorted(jnp.cumsum(sizes), jnp.arange(rows * top), side="right").astype(jnp.int32)
    table = items.reshape(top, rows).T
    table = table[jax.random.permutation(jax.random.fold_in(own, 1), rows)]
    turn = jax.random.randint(jax.random.fold_in(own, 2), (rows, 1), 0, top)
    return jnp.take_along_axis(table, (jnp.arange(top)[None, :] + turn) % top, axis=1)


def portions_of(count, total, bound, lean, full):
    loads = [(1 << 20) // math.isqrt(grade ** lean) + 1 for grade in range(1, count + 1)]
    largest = bound if full else min(bound, max(-(-total // count), total * loads[0] // sum(loads)))
    least = 1 if total - largest >= count - 1 else 0
    counts, spare = [largest] + [least] * (count - 1), total - largest - least * (count - 1)
    while spare > 0:
        free = [i for i in range(1, count) if counts[i] < largest] or [i for i in range(1, count) if counts[i] < bound]
        mass, remaining = sum([loads[i] for i in free]), spare
        for i in free:
            more = min(bound - counts[i], max(1, remaining * loads[i] // mass), spare)
            counts[i] = counts[i] + more
            spare = spare - more
    return np.array(counts)


def normal_values(stream_key, extent, scale, reach, pieces=(), kind=jnp.bfloat16):
    entries = scale * jax.random.normal(stream_key, extent, jnp.float32)
    if pieces:
        entries = entries * steps_of(stream_key, extent, pieces, -0.22, 0.18)
    return jnp.clip(entries, -reach, reach).astype(kind)


def setup_inputs(seed: int = 0) -> dict:
    splits = jax.random.split(jax.random.key(seed), 14)
    queries = draw_queries(jax.random.fold_in(splits[13], 71), 0)
    keys = draw_keys(jax.random.fold_in(splits[13], 71), 0)
    values = normal_values(splits[2], (SEQ, KV_HEADS, VD), 1.0, 6.0, ((0, 64), (1, 4)))
    mix_scale = jnp.clip(0.3 + 0.5 * jax.random.uniform(splits[3], (HEADS,), jnp.float32) ** steps_of(splits[3], (HEADS,), ((0, 4),), -0.2, 0.2), 0.3, 0.8)
    head_gain = jnp.clip(1.0 + 0.18 * jax.random.normal(splits[4], (VD,), jnp.float32), 0.1, 1.9)
    out_weight = normal_values(splits[5], (HEADS, VD, D), (HEADS * VD) ** -0.5, 0.1875, ((0, 4),))
    moe_input = normal_values(splits[6], (TOKENS_M, D), 1.0, 6.0, ((0, 256),))
    norm_gain = jnp.clip(1.0 + 0.18 * jax.random.normal(splits[7], (D,), jnp.float32), 0.1, 1.9)
    routes_keys = jax.random.split(jax.random.fold_in(splits[8], 1), TOKENS_M // TOK_M)
    routes_turns = jax.random.permutation(jax.random.fold_in(splits[8], 3), TOKENS_M // TOK_M)
    routes = jax.vmap(lambda own, number: deal_out(jax.random.fold_in(splits[8], 2), own, number, TOK_M, EXPERTS, TOPK, CAP, 1))(routes_keys, routes_turns).reshape((TOKENS_M, TOPK))
    route_weights = jnp.clip(0.2 + 0.8 * jax.random.uniform(splits[9], (TOKENS_M, TOPK), jnp.float32) ** steps_of(splits[9], (TOKENS_M, TOPK), ((0, 256),), -0.2, 0.2), 0.2, 1.0)
    gate_weight = normal_values(splits[10], (EXPERTS, D, FFE), D ** -0.5, 0.125, ((0, 64), (2, 4)))
    up_weight = normal_values(splits[11], (EXPERTS, D, FFE), D ** -0.5, 0.125, ((0, 64), (2, 4)))
    down_weight = normal_values(splits[12], (EXPERTS, FFE, D), FFE ** -0.5, 0.09375, ((0, 64), (1, 4)))
    return dict(queries=queries, keys=keys, values=values, mix_scale=mix_scale, head_gain=head_gain, out_weight=out_weight, moe_input=moe_input, norm_gain=norm_gain, routes=routes, route_weights=route_weights, gate_weight=gate_weight, up_weight=up_weight, down_weight=down_weight)


def reference(queries, keys, values, mix_scale, head_gain, out_weight, moe_input, norm_gain, routes, route_weights, gate_weight, up_weight, down_weight):
    group_size = HEADS // KV_HEADS
    key_table = jnp.repeat(keys.reshape(SEQ, KV_HEADS, 2, HD), group_size, axis=1).astype(jnp.float32)
    value_table = jnp.repeat(values, group_size, axis=1).astype(jnp.float32)
    query_table = queries.reshape(SEQ, HEADS, 2, HD)
    key_positions = jnp.arange(SEQ, dtype=jnp.int32)

    def attend_block(block_id):
        first_row = block_id * TA
        query_block = lax.dynamic_slice_in_dim(query_table, first_row, TA, 0).astype(jnp.float32)
        scores = jnp.einsum('thmd,shmd->hmts', query_block, key_table) / math.sqrt(HD)
        positions = first_row + jnp.arange(TA, dtype=jnp.int32)
        visible = key_positions[None, :] <= positions[:, None]
        scores = jnp.where(visible, scores, -jnp.inf)
        row_peak = lax.optimization_barrier(jnp.max(scores, axis=-1, keepdims=True))
        weights = jnp.where(visible, jnp.exp(scores - row_peak), 0.0)
        totals = lax.optimization_barrier(jnp.sum(weights, axis=-1))
        rounded = lax.optimization_barrier(weights.astype(jnp.bfloat16)).astype(jnp.float32)
        numerator = jnp.einsum('hmts,shv->hmtv', rounded, value_table)
        blended = numerator[:, 0] / totals[:, 0, :, None] - mix_scale[:, None, None] * (numerator[:, 1] / totals[:, 1, :, None])
        normed = blended * lax.rsqrt(lax.optimization_barrier(jnp.mean(blended * blended, axis=-1, keepdims=True)) + 1e-05) * head_gain
        return jnp.transpose(normed.astype(jnp.bfloat16), (1, 0, 2))
    attended = lax.map(attend_block, jnp.arange(N_EP, dtype=jnp.int32)).reshape(SEQ, HEADS * VD)
    heads_group = HEADS // N_TP
    attn_sum = jnp.zeros((SEQ, D), jnp.float32)
    for member in range(N_TP):
        columns = attended[:, member * heads_group * VD:(member + 1) * heads_group * VD]
        weight_rows = out_weight[member * heads_group:(member + 1) * heads_group].reshape(heads_group * VD, D)
        head_part = jnp.dot(columns, weight_rows, preferred_element_type=jnp.float32).astype(jnp.bfloat16)
        attn_sum = attn_sum + head_part.astype(jnp.float32)
    attn_out = attn_sum.astype(jnp.bfloat16)
    widened = moe_input.astype(jnp.float32)
    normed_in = (widened * lax.rsqrt(lax.optimization_barrier(jnp.mean(widened * widened, axis=-1, keepdims=True)) + 1e-06) * norm_gain).astype(jnp.bfloat16)
    padded = jnp.concatenate([normed_in, jnp.zeros((1, D), jnp.bfloat16)], axis=0)
    limit = TOKENS_M // TOK_M * CAP
    width = FFE // N_TP

    def expert_step(running, expert_id):
        matches = routes == expert_id
        chosen = jnp.any(matches, axis=1)
        weight_row = lax.optimization_barrier(jnp.sum(jnp.where(matches, route_weights, 0.0), axis=1))
        row_ids = jnp.nonzero(chosen, size=limit, fill_value=TOKENS_M)[0].astype(jnp.int32)
        selected = padded[row_ids]
        gate_proj = jnp.dot(selected, gate_weight[expert_id], preferred_element_type=jnp.float32)
        up_proj = jnp.dot(selected, up_weight[expert_id], preferred_element_type=jnp.float32)
        hidden = (jax.nn.silu(gate_proj) * up_proj).astype(jnp.bfloat16)
        down_rows = down_weight[expert_id]
        summed = jnp.zeros((limit, D), jnp.float32)
        for member in range(N_TP):
            part = jnp.dot(hidden[:, member * width:(member + 1) * width], down_rows[member * width:(member + 1) * width], preferred_element_type=jnp.float32)
            summed = summed + part.astype(jnp.bfloat16).astype(jnp.float32)
        expert_out = summed.astype(jnp.bfloat16)
        row_weights = jnp.concatenate([weight_row, jnp.zeros((1,), jnp.float32)])[row_ids]
        running = running.at[row_ids].add(row_weights[:, None] * expert_out.astype(jnp.float32), mode='drop')
        return (running, None)
    collected, _ = lax.scan(expert_step, jnp.zeros((TOKENS_M, D), jnp.float32), jnp.arange(EXPERTS, dtype=jnp.int32))
    return (attn_out, collected.astype(jnp.bfloat16))
```

```python
import functools

import jax
import jax.numpy as jnp
from jax import lax
from jax.experimental import pallas as pl
from jax.experimental.pallas import tpu as pltpu
from jax.sharding import Mesh
from jax.sharding import PartitionSpec as P

EP = ("ep_0", "ep_1", "ep_2")
EP_TP = ("ep_0", "ep_1", "ep_2", "tp")
MESH = pl.DeviceIdType.MESH

NZ, NY, NC, NX = 8, 4, 2, 4
CHUNKS = NY
BLOCKS = NZ * NC
CAP = 4
QUARTERS = 4
GROUP = BLOCKS * CAP
NEG_LARGE = -1e30
F32 = jnp.float32
BF16 = jnp.bfloat16


def dz_order():
    return (1, 7, 2, 6, 3, 5, 4, 0)


def kernel(
    outbound,
    q_ref,
    k_ref,
    v_ref,
    ow_ref,
    comb_ref,
    mix_ref,
    gain_ref,
    gw_hbm,
    uw_hbm,
    dw_hbm,
    attn_o,
    moe_o,
    gw,
    uw,
    dw,
    kbuf,
    vbuf,
    perm,
    perm_t,
    arr,
    xb,
    hid,
    part,
    opp,
    fin,
    back,
    ret,
    rows_ref,
    m_ref,
    l_ref,
    acc_ref,
    att_ref,
    ap,
    ar,
    w_sem,
    kv_own,
    kv_send,
    kv_recv,
    a_send,
    a_recv,
    x_send,
    x_recv,
    f_send,
    f_recv,
    s1_send,
    s1_recv,
    s2_send,
    fin_recv,
    b_send,
    r_recv,
    at_send,
    at_recv,
):
    z = lax.axis_index("ep_0")
    y = lax.axis_index("ep_1")
    c = lax.axis_index("ep_2")
    x = lax.axis_index("tp")
    me = z * (NY * NC) + y * NC + c
    right = {"tp": lax.rem(x + 1, NX)}
    left = {"tp": lax.rem(x + NX - 1, NX)}
    y_up = {"ep_1": lax.rem(y + 1, NY)}
    y_down = {"ep_1": lax.rem(y + NY - 1, NY)}
    ym1 = lax.rem(y + NY - 1, NY)
    yp1 = lax.rem(y + 1, NY)
    partner = {"ep_2": 1 - c}

    def rcopy(src, dst, ssem, rsem, dev):
        return pltpu.make_async_remote_copy(
            src_ref=src, dst_ref=dst, send_sem=ssem, recv_sem=rsem, device_id=dev, device_id_type=MESH
        )

    weights = [
        pltpu.make_async_copy(s, d, w_sem.at[i]) for i, (s, d) in enumerate(((gw_hbm, gw), (uw_hbm, uw), (dw_hbm, dw)))
    ]
    for copy in weights:
        copy.start()

    def send_rows(g, carry):
        for dz in dz_order():
            for dc in range(NC):
                i = dz * NC + dc

                def go():
                    dev = {
                        "ep_0": lax.rem(z + dz, NZ),
                        "ep_1": lax.rem(y + g, NY),
                        "ep_2": (1 - c) if dc else c,
                    }
                    rcopy(outbound.at[g, i], arr.at[g, i], a_send.at[0], a_recv.at[g], dev).start()

                if i == 0:
                    pl.when(g > 0)(go)
                else:
                    go()
        return carry

    lax.fori_loop(0, CHUNKS, send_rows, 0)
    pltpu.make_async_copy(outbound.at[0, 0], arr.at[0, 0], a_recv.at[0]).start()

    kv = ((k_ref, kbuf, 0), (v_ref, vbuf, 1))
    kv_z = []
    for ref, buf, j in kv:
        pltpu.make_async_copy(ref, buf.at[z, y, c], kv_own.at[j]).start()
        for dz in (1, 7, 2, 6, 3, 5, 4):
            copy = rcopy(ref, buf.at[z, y, c], kv_send.at[0, j], kv_recv.at[0, j], {"ep_0": lax.rem(z + dz, NZ)})
            copy.start()

    def kv_y():
        for ref, buf, j in kv:
            pltpu.make_async_copy(ref, buf.at[z, y, c], kv_own.at[j]).wait()
            pltpu.make_async_copy(
                buf.at[pl.ds(0, NZ - 1), y, c], buf.at[pl.ds(0, NZ - 1), y, c], kv_recv.at[0, j]
            ).wait()
            rcopy(buf.at[:, y, c], buf.at[:, y, c], kv_send.at[1, j], kv_recv.at[1, j], y_up).start()
            rcopy(buf.at[:, y, c], buf.at[:, y, c], kv_send.at[2, j], kv_recv.at[2, j], y_down).start()

    half = NZ // 2

    def kv_y2():
        for ref, buf, j in kv:
            rcopy(buf.at[:, ym1, c], buf.at[:, ym1, c], kv_send.at[1, j], kv_recv.at[1, j], y_up).wait_recv()
            lo = buf.at[pl.ds(0, half), ym1, c]
            rcopy(lo, lo, kv_send.at[3, j], kv_recv.at[3, j], y_up).start()
            rcopy(buf.at[:, yp1, c], buf.at[:, yp1, c], kv_send.at[2, j], kv_recv.at[2, j], y_down).wait_recv()
            hi = buf.at[pl.ds(half, half), yp1, c]
            rcopy(hi, hi, kv_send.at[4, j], kv_recv.at[4, j], y_down).start()

    def kv_core():
        yo = lax.rem(y + 2, NY)
        for ref, buf, j in kv:
            lo = buf.at[pl.ds(0, half), yo, c]
            rcopy(lo, lo, kv_send.at[3, j], kv_recv.at[3, j], y_up).wait_recv()
            hi = buf.at[pl.ds(half, half), yo, c]
            rcopy(hi, hi, kv_send.at[4, j], kv_recv.at[4, j], y_down).wait_recv()
            rcopy(buf.at[:, :, c], buf.at[:, :, c], kv_send.at[5, j], kv_recv.at[5, j], partner).start()

    size = BLOCKS * QUARTERS * CAP
    r_io = lax.broadcasted_iota(jnp.int32, (size, size), 0)
    c_io = lax.broadcasted_iota(jnp.int32, (size, size), 1)

    def packed_place(r):
        return (r % GROUP) // CAP * (QUARTERS * CAP) + r // GROUP * CAP + r % CAP

    perm[...] = (packed_place(r_io) == c_io).astype(BF16)
    perm_t[...] = (packed_place(c_io) == r_io).astype(BF16)
    width = outbound.shape[-1]

    def relayout_in(src, g, store):
        tile = src[g].reshape(size, width)
        turned = jnp.dot(perm[...], tile, preferred_element_type=F32).astype(BF16)
        for kq in range(QUARTERS):
            store(kq, turned[kq * GROUP : (kq + 1) * GROUP])

    def gather_first(g):
        pltpu.make_async_copy(arr.at[g], arr.at[g], a_recv.at[g]).wait()

        def store(kq, value):
            xb[g, 0, :, kq * width : (kq + 1) * width] = value

        relayout_in(arr, g, store)
        rcopy(xb.at[g, 0], xb.at[g, 1], x_send.at[0, g], x_recv.at[0, g], right).start()
        rcopy(xb.at[g, 0], xb.at[g, 2], x_send.at[1, g], x_recv.at[1, g], left).start()

    top, low = pl.ds(0, GROUP // 2), pl.ds(GROUP // 2, GROUP // 2)

    def gather_second(g):
        rcopy(xb.at[g, 0], xb.at[g, 1], x_send.at[0, g], x_recv.at[0, g], right).wait_recv()
        rcopy(xb.at[g, 1, top], xb.at[g, 3, top], f_send.at[0, g], f_recv.at[0, g], right).start()
        rcopy(xb.at[g, 0], xb.at[g, 2], x_send.at[1, g], x_recv.at[1, g], left).wait_recv()
        rcopy(xb.at[g, 2, low], xb.at[g, 3, low], f_send.at[1, g], f_recv.at[1, g], left).start()

    ffe = gw.shape[1]
    model = gw.shape[0]
    rows = NX * GROUP

    def experts(g):
        rcopy(xb.at[g, 1, top], xb.at[g, 3, top], f_send.at[0, g], f_recv.at[0, g], right).wait_recv()
        rcopy(xb.at[g, 2, low], xb.at[g, 3, low], f_send.at[1, g], f_recv.at[1, g], left).wait_recv()

        @pl.when(g == 0)
        def _():
            for copy in weights:
                copy.wait()

        inputs = xb[g].reshape(rows, model)
        for n in range(0, ffe, 256):
            w = min(256, ffe - n)
            gate = jnp.dot(inputs, gw[:, n : n + w], preferred_element_type=F32)
            up = jnp.dot(inputs, uw[:, n : n + w], preferred_element_type=F32)
            hid[:, n : n + w] = (gate / (1.0 + jnp.exp(-gate)) * up).astype(BF16)
        hidden = hid[...]
        for n in range(0, model, 256):
            part[g, :, :, n : n + 256] = (
                jnp.dot(hidden, dw[:, n : n + 256], preferred_element_type=F32).astype(BF16).reshape(NX, GROUP, 256)
            )
        rcopy(part.at[g, 3, top], opp.at[g, 0], s1_send.at[0, g], s1_recv.at[0, g], right).start()
        rcopy(part.at[g, 3, low], opp.at[g, 1], s1_send.at[1, g], s1_recv.at[1, g], left).start()
        rcopy(part.at[g, 2, low], fin.at[g, 0, low], s2_send.at[0, g], fin_recv.at[0, g], right).start()
        rcopy(part.at[g, 1, top], fin.at[g, 1, top], s2_send.at[1, g], fin_recv.at[1, g], left).start()

    def sum_second(g):
        rcopy(part.at[g, 3, top], opp.at[g, 0], s1_send.at[0, g], s1_recv.at[0, g], right).wait_recv()
        part[g, 2, : GROUP // 2] = (part[g, 2, : GROUP // 2].astype(F32) + opp[g, 0].astype(F32)).astype(BF16)
        rcopy(part.at[g, 2, top], fin.at[g, 0, top], s2_send.at[2, g], fin_recv.at[2, g], right).start()
        rcopy(part.at[g, 3, low], opp.at[g, 1], s1_send.at[1, g], s1_recv.at[1, g], left).wait_recv()
        part[g, 1, GROUP // 2 :] = (part[g, 1, GROUP // 2 :].astype(F32) + opp[g, 1].astype(F32)).astype(BF16)
        rcopy(part.at[g, 1, low], fin.at[g, 1, low], s2_send.at[3, g], fin_recv.at[3, g], left).start()

    def sum_last(g):
        rcopy(part.at[g, 2, low], fin.at[g, 0, low], s2_send.at[0, g], fin_recv.at[0, g], right).wait_recv()
        rcopy(part.at[g, 1, top], fin.at[g, 1, top], s2_send.at[1, g], fin_recv.at[1, g], left).wait_recv()
        rcopy(part.at[g, 2, top], fin.at[g, 0, top], s2_send.at[2, g], fin_recv.at[2, g], right).wait_recv()
        rcopy(part.at[g, 1, low], fin.at[g, 1, low], s2_send.at[3, g], fin_recv.at[3, g], left).wait_recv()
        total = (part[g, 0].astype(F32) + fin[g, 0].astype(F32) + fin[g, 1].astype(F32)).astype(BF16)
        tall = jnp.concatenate([total[:, kq * width : (kq + 1) * width] for kq in range(QUARTERS)], axis=0)
        back[g] = (
            jnp.dot(perm_t[...], tall, preferred_element_type=F32).astype(BF16).reshape(BLOCKS, QUARTERS * CAP, width)
        )
        for dz in dz_order():
            for dc in range(NC):
                i = dz * NC + dc

                def go():
                    dev = {
                        "ep_0": lax.rem(z + NZ - dz, NZ),
                        "ep_1": lax.rem(y + NY - g, NY),
                        "ep_2": (1 - c) if dc else c,
                    }
                    rcopy(back.at[g, i], ret.at[g, i], b_send.at[0], r_recv.at[g], dev).start()

                if i == 0:
                    pl.when(g > 0)(go)

                    @pl.when(g == 0)
                    def _():
                        pltpu.make_async_copy(back.at[0, 0], ret.at[0, 0], r_recv.at[0]).start()

                else:
                    go()

    ta = q_ref.shape[1]
    heads = q_ref.shape[0] // 2
    span = 2 * NC * ta

    def attend():
        for ref, buf, j in kv:
            rcopy(
                buf.at[:, :, 1 - c], buf.at[:, :, 1 - c], kv_send.at[5, j], kv_recv.at[5, j], partner
            ).wait_recv()
        m_ref[...] = jnp.full(m_ref.shape, NEG_LARGE, F32)
        l_ref[...] = jnp.zeros(l_ref.shape, F32)
        acc_ref[...] = jnp.zeros(acc_ref.shape, F32)

        def chunk(t, masked):
            zz = t // 2
            yh = t % 2
            kc = kbuf[zz, pl.ds(yh * 2, 2)].reshape(span, kbuf.shape[-1])
            vc = vbuf[zz, pl.ds(yh * 2, 2)].reshape(span, vbuf.shape[-1])
            for r in range(2 * heads):
                s = lax.dot_general(q_ref[r], kc, (((1,), (1,)), ((), ())), preferred_element_type=F32)
                if masked:
                    kpos = t * span + lax.broadcasted_iota(jnp.int32, s.shape, 1)
                    qpos = me * ta + lax.broadcasted_iota(jnp.int32, s.shape, 0)
                    s = jnp.where(kpos <= qpos, s, NEG_LARGE)
                old = m_ref[r][:, :1]
                new = jnp.maximum(old, jnp.max(s, axis=1, keepdims=True))
                p = jnp.exp(s - new)
                scale = jnp.exp(old - new)
                l_ref[r] = jnp.broadcast_to(
                    l_ref[r][:, :1] * scale + jnp.sum(p, axis=1, keepdims=True), l_ref.shape[1:]
                )
                m_ref[r] = jnp.broadcast_to(new, m_ref.shape[1:])
                acc_ref[r] = acc_ref[r] * scale + jnp.dot(p.astype(BF16), vc, preferred_element_type=F32)

        last = me // (2 * NC)

        def step(t, carry):
            chunk(t, False)
            return carry

        lax.fori_loop(0, last, step, 0)
        chunk(last, True)
        for h in range(heads):
            blended = acc_ref[h] / l_ref[h] - mix_ref[h] * (acc_ref[heads + h] / l_ref[heads + h])
            normed = (
                blended * lax.rsqrt(jnp.mean(blended * blended, axis=1, keepdims=True) + 1e-05) * gain_ref[...]
            ).astype(BF16)
            att_ref[:, :, h * 128 : (h + 1) * 128] = normed.reshape(NX, ta // NX, 128)
        for r in range(NX):
            j = lax.rem(x + r, NX)
            ap[r] = jnp.dot(att_ref[j], ow_ref[...], preferred_element_type=F32).astype(BF16)
            if r:
                rcopy(ap.at[r], ar.at[r - 1], at_send.at[r - 1], at_recv.at[r - 1], {"tp": j}).start()

    def main(s, carry):
        @pl.when((s >= 4) & (s < CHUNKS + 4))
        def _():
            sum_last(s - 4)

        @pl.when((s >= 3) & (s < CHUNKS + 3))
        def _():
            sum_second(s - 3)

        @pl.when(s < CHUNKS)
        def _():
            gather_first(s)

        @pl.when((s >= 1) & (s < CHUNKS + 1))
        def _():
            gather_second(s - 1)

        pl.when(s == 1)(kv_y)
        pl.when(s == 2)(kv_y2)
        pl.when(s == 3)(kv_core)

        @pl.when((s >= 2) & (s < CHUNKS + 2))
        def _():
            experts(s - 2)

        pl.when(s == CHUNKS + 1)(attend)
        return carry

    lax.fori_loop(0, CHUNKS + 4, main, 0)

    for r in range(1, NX):
        rcopy(ap.at[r], ar.at[r - 1], at_send.at[r - 1], at_recv.at[r - 1], right).wait_recv()
    total = ap[0].astype(F32)
    for r in range(1, NX):
        total = total + ar[r - 1].astype(F32)
    attn_o[...] = total.astype(BF16)

    def collect(g, carry):
        pltpu.make_async_copy(ret.at[g], ret.at[g], r_recv.at[g]).wait()

        def store(kq, value):
            rows_ref[pl.ds(pl.multiple_of(g * GROUP, GROUP), GROUP), kq * width : (kq + 1) * width] = value

        relayout_in(ret, g, store)
        return carry

    lax.fori_loop(0, CHUNKS, collect, 0)
    tokens = moe_o.shape[0]
    for kq in range(QUARTERS):
        both = jnp.dot(comb_ref[...], rows_ref[:, kq * width : (kq + 1) * width], preferred_element_type=F32)
        moe_o[:, kq * width : (kq + 1) * width] = (both[:tokens] + both[tokens:]).astype(BF16)

    for g in range(CHUNKS):
        for copy in (
            rcopy(xb.at[g, 0], xb.at[g, 1], x_send.at[0, g], x_recv.at[0, g], right),
            rcopy(xb.at[g, 0], xb.at[g, 2], x_send.at[1, g], x_recv.at[1, g], left),
            rcopy(xb.at[g, 1, top], xb.at[g, 3, top], f_send.at[0, g], f_recv.at[0, g], right),
            rcopy(xb.at[g, 2, low], xb.at[g, 3, low], f_send.at[1, g], f_recv.at[1, g], left),
            rcopy(part.at[g, 3, top], opp.at[g, 0], s1_send.at[0, g], s1_recv.at[0, g], right),
            rcopy(part.at[g, 3, low], opp.at[g, 1], s1_send.at[1, g], s1_recv.at[1, g], left),
            rcopy(part.at[g, 2, low], fin.at[g, 0, low], s2_send.at[0, g], fin_recv.at[0, g], right),
            rcopy(part.at[g, 1, top], fin.at[g, 1, top], s2_send.at[1, g], fin_recv.at[1, g], left),
            rcopy(part.at[g, 2, top], fin.at[g, 0, top], s2_send.at[2, g], fin_recv.at[2, g], right),
            rcopy(part.at[g, 1, low], fin.at[g, 1, low], s2_send.at[3, g], fin_recv.at[3, g], left),
        ):
            copy.wait_send()
    for r in range(1, NX):
        rcopy(ap.at[r], ar.at[r - 1], at_send.at[r - 1], at_recv.at[r - 1], right).wait_send()
    for ref, buf, j in kv:
        seven = buf.at[pl.ds(0, NZ - 1), y, c]
        rcopy(seven, seven, kv_send.at[0, j], kv_recv.at[0, j], y_up).wait_send()
        for n in (1, 2):
            rcopy(buf.at[:, y, c], buf.at[:, y, c], kv_send.at[n, j], kv_recv.at[n, j], y_up).wait_send()
        for n in (3, 4):
            lo = buf.at[pl.ds(0, half), y, c]
            rcopy(lo, lo, kv_send.at[n, j], kv_recv.at[n, j], y_up).wait_send()
        rcopy(buf.at[:, :, c], buf.at[:, :, c], kv_send.at[5, j], kv_recv.at[5, j], partner).wait_send()
    for sem, buf in ((a_send, outbound), (b_send, back)):
        for g in range(CHUNKS):
            blocks = buf.at[g, pl.ds(1, BLOCKS - 1)] if g == 0 else buf.at[g]
            rcopy(blocks, blocks, sem.at[0], r_recv.at[g], right).wait_send()


def body(
    queries,
    keys,
    values,
    mix_scale,
    head_gain,
    out_weight,
    moe_input,
    norm_gain,
    routes,
    route_weights,
    gate_weight,
    up_weight,
    down_weight,
):
    ta, heads, qd = queries.shape
    tok, model = moe_input.shape
    ffe = gate_weight.shape[2]
    vd = values.shape[2]
    width = model // QUARTERS
    z = lax.axis_index("ep_0")
    y = lax.axis_index("ep_1")
    c = lax.axis_index("ep_2")

    widened = moe_input.astype(F32)
    normed = (
        widened * lax.rsqrt(jnp.mean(widened * widened, axis=-1, keepdims=True) + 1e-06) * norm_gain
    ).astype(BF16)
    flat = routes.reshape(-1)
    count = flat.shape[0]
    places = jnp.arange(count, dtype=jnp.int32)
    earlier = (flat[:, None] == flat[None, :]) & (places[None, :] < places[:, None])
    rank = jnp.sum(earlier.astype(jnp.int32), axis=1).reshape(routes.shape)
    ez, ey, ec = routes // (NY * NC), (routes // NC) % NY, routes % NC
    offset = ((ey - y) % NY) * BLOCKS + ((ez - z) % NZ) * NC + (ec + c) % NC
    slot = offset * CAP + rank
    slots = NY * BLOCKS * CAP

    r = jnp.arange(slots * QUARTERS, dtype=jnp.int32)
    r_slot = r // (QUARTERS * CAP) * CAP + r % CAP
    r_quarter = (r // CAP) % QUARTERS
    col = jnp.arange(QUARTERS * tok, dtype=jnp.int32)
    col_quarter = col // tok
    col_slot = jnp.tile(slot, (QUARTERS, 1))
    chosen = (r_slot[:, None] == col_slot[None, :, 0]) | (r_slot[:, None] == col_slot[None, :, 1])
    dispatch = (chosen & (r_quarter[:, None] == col_quarter[None, :])).astype(BF16)
    stacked = normed.reshape(tok, QUARTERS, width).transpose(1, 0, 2).reshape(QUARTERS * tok, width)
    outbound = jnp.dot(dispatch, stacked, preferred_element_type=F32).astype(BF16)
    outbound = outbound.reshape(CHUNKS, BLOCKS, QUARTERS * CAP, width)

    places = jnp.arange(slots, dtype=jnp.int32)
    comb = jnp.sum(
        jnp.where(slot[:, :, None] == places[None, None, :], route_weights[:, :, None], 0.0), axis=1
    )
    high = comb.astype(BF16)
    comb = jnp.concatenate([high, (comb - high.astype(F32)).astype(BF16)], axis=0)

    scaled = (queries.astype(F32) * (1.0 / (qd // 2) ** 0.5)).astype(BF16).transpose(1, 0, 2)
    lane = jnp.arange(qd, dtype=jnp.int32)[None, None, :]
    zero = jnp.zeros((), BF16)
    q_all = jnp.concatenate(
        [jnp.where(lane < qd // 2, scaled, zero), jnp.where(lane < qd // 2, zero, scaled)], axis=0
    )

    vmem = pl.BlockSpec(memory_space=pltpu.VMEM)
    hbm = pl.BlockSpec(memory_space=pl.ANY)
    dma = pltpu.SemaphoreType.DMA
    size = BLOCKS * QUARTERS * CAP
    attn_out, moe_out = pl.pallas_call(
        kernel,
        out_shape=(
            jax.ShapeDtypeStruct((ta // NX, model), BF16),
            jax.ShapeDtypeStruct((tok, model), BF16),
        ),
        in_specs=[vmem] * 6 + [pl.BlockSpec(memory_space=pltpu.SMEM), vmem] + [hbm] * 3,
        out_specs=(vmem, vmem),
        scratch_shapes=[
            pltpu.VMEM((model, ffe), BF16),
            pltpu.VMEM((model, ffe), BF16),
            pltpu.VMEM((ffe, model), BF16),
            pltpu.VMEM((NZ, NY, NC, ta, qd), BF16),
            pltpu.VMEM((NZ, NY, NC, ta, vd), BF16),
            pltpu.VMEM((size, size), BF16),
            pltpu.VMEM((size, size), BF16),
            pltpu.VMEM((CHUNKS, BLOCKS, QUARTERS * CAP, width), BF16),
            pltpu.VMEM((CHUNKS, NX, GROUP, model), BF16),
            pltpu.VMEM((NX * GROUP, ffe), BF16),
            pltpu.VMEM((CHUNKS, NX, GROUP, model), BF16),
            pltpu.VMEM((CHUNKS, 2, GROUP // 2, model), BF16),
            pltpu.VMEM((CHUNKS, 2, GROUP, model), BF16),
            pltpu.VMEM((CHUNKS, BLOCKS, QUARTERS * CAP, width), BF16),
            pltpu.VMEM((CHUNKS, BLOCKS, QUARTERS * CAP, width), BF16),
            pltpu.VMEM((slots, model), BF16),
            pltpu.VMEM((2 * heads, ta, 128), F32),
            pltpu.VMEM((2 * heads, ta, 128), F32),
            pltpu.VMEM((2 * heads, ta, vd), F32),
            pltpu.VMEM((NX, ta // NX, heads * vd), BF16),
            pltpu.VMEM((NX, ta // NX, model), BF16),
            pltpu.VMEM((NX - 1, ta // NX, model), BF16),
            dma((3,)),
            dma((2,)),
            dma((6, 2)),
            dma((6, 2)),
            dma((1,)),
            dma((CHUNKS,)),
            dma((2, CHUNKS)),
            dma((2, CHUNKS)),
            dma((2, CHUNKS)),
            dma((2, CHUNKS)),
            dma((2, CHUNKS)),
            dma((2, CHUNKS)),
            dma((4, CHUNKS)),
            dma((4, CHUNKS)),
            dma((1,)),
            dma((CHUNKS,)),
            dma((NX - 1,)),
            dma((NX - 1,)),
        ],
        compiler_params=pltpu.CompilerParams(has_side_effects=True, vmem_limit_bytes=62 * 1024 * 1024),
    )(
        outbound,
        q_all,
        keys.reshape(ta, qd),
        values.reshape(ta, vd),
        out_weight.reshape(heads * vd, model),
        comb,
        mix_scale,
        head_gain.reshape(1, vd),
        gate_weight[0],
        up_weight[0],
        down_weight[0],
    )
    return (attn_out, moe_out)


def solution(mesh):
    split = Mesh(mesh.devices.reshape(NZ, NY, NC, NX), EP_TP)
    placed = (
        P(EP, "tp", None),
        P(EP, "tp", None),
        P(EP, "tp", None),
        P("tp"),
        P(),
        P("tp", None, None),
        P(EP_TP, None),
        P(),
        P(EP_TP, None),
        P(EP_TP, None),
        P(EP, None, "tp"),
        P(EP, None, "tp"),
        P(EP, "tp", None),
    )
    return jax.shard_map(
        body,
        mesh=split,
        in_specs=placed,
        out_specs=(P(EP_TP, None), P(EP_TP, None)),
        check_vma=False,
    )
```

```python
import functools

import jax
import jax.numpy as jnp
from jax import lax
from jax.experimental import pallas as pl
from jax.experimental.pallas import tpu as pltpu
from jax.sharding import Mesh
from jax.sharding import PartitionSpec as P

EP = ("ep_0", "ep_1", "ep_2")
EP_TP = ("ep_0", "ep_1", "ep_2", "tp")
MESH = pl.DeviceIdType.MESH

NZ, NY, NC, NX = 8, 4, 2, 4
CHUNKS = NY
BLOCKS = NZ * NC
CAP = 4
QUARTERS = 4
GROUP = BLOCKS * CAP
NEG_LARGE = -1e30
F32 = jnp.float32
BF16 = jnp.bfloat16


def dz_order():
    return (1, 7, 2, 6, 3, 5, 4, 0)


def kernel(
    tok_ref,
    ng_ref,
    routes_ref,
    rw_ref,
    q_in,
    k_ref,
    v_ref,
    mix_ref,
    gain_ref,
    ow_hbm,
    gw_hbm,
    uw_hbm,
    dw_hbm,
    attn_o,
    moe_o,
    gw,
    uw,
    dw,
    ow_ref,
    outbound,
    q_ref,
    comb_ref,
    kbuf,
    vbuf,
    perm,
    perm_t,
    arr,
    xb,
    hid,
    part,
    opp,
    fin,
    back,
    ret,
    rows_ref,
    m_ref,
    acc_ref,
    att_ref,
    ap,
    ar,
    w_sem,
    kv_own,
    z_send,
    z_recv,
    y_send,
    y_recv,
    h_send,
    h_recv,
    c_send,
    c_recv,
    a_send,
    a_recv,
    x_send,
    x_recv,
    f_send,
    f_recv,
    s1_send,
    s1_recv,
    s2_send,
    fin_recv,
    b_send,
    r_recv,
    at_send,
    at_recv,
):
    z = lax.axis_index("ep_0")
    y = lax.axis_index("ep_1")
    c = lax.axis_index("ep_2")
    x = lax.axis_index("tp")
    me = z * (NY * NC) + y * NC + c
    right = {"tp": lax.rem(x + 1, NX)}
    left = {"tp": lax.rem(x + NX - 1, NX)}
    y_up = {"ep_1": lax.rem(y + 1, NY)}
    y_down = {"ep_1": lax.rem(y + NY - 1, NY)}
    ym1 = lax.rem(y + NY - 1, NY)
    yp1 = lax.rem(y + 1, NY)
    partner = {"ep_2": 1 - c}

    def rcopy(src, dst, ssem, rsem, dev):
        return pltpu.make_async_remote_copy(
            src_ref=src, dst_ref=dst, send_sem=ssem, recv_sem=rsem, device_id=dev, device_id_type=MESH
        )

    barrier = pltpu.get_barrier_semaphore()

    def greet(g, carry):
        for dz in range(NZ):
            for dc in range(NC):

                def go():
                    pl.semaphore_signal(
                        barrier,
                        inc=1,
                        device_id={
                            "ep_0": lax.rem(z + dz, NZ),
                            "ep_1": lax.rem(y + g, NY),
                            "ep_2": (1 - c) if dc else c,
                        },
                        device_id_type=MESH,
                    )

                if dz == 0 and dc == 0:
                    pl.when(g > 0)(go)
                else:
                    go()
        return carry

    lax.fori_loop(0, CHUNKS, greet, 0)
    for r in range(1, NX):
        pl.semaphore_signal(barrier, inc=1, device_id={"tp": lax.rem(x + r, NX)}, device_id_type=MESH)

    kv = ((k_ref, kbuf, 0), (v_ref, vbuf, 1))
    for ref, buf, j in kv:
        pltpu.make_async_copy(ref, buf.at[z, y, c], kv_own.at[j]).start()
    weights = [
        pltpu.make_async_copy(s, d, w_sem.at[i])
        for i, (s, d) in enumerate(((gw_hbm, gw), (uw_hbm, uw), (dw_hbm, dw), (ow_hbm, ow_ref)))
    ]
    for copy in weights:
        copy.start()

    size = BLOCKS * QUARTERS * CAP
    r_io = lax.broadcasted_iota(jnp.int32, (size, size), 0)
    c_io = lax.broadcasted_iota(jnp.int32, (size, size), 1)

    def packed_place(r):
        return (r % GROUP) // CAP * (QUARTERS * CAP) + r // GROUP * CAP + r % CAP

    perm[...] = (packed_place(r_io) == c_io).astype(BF16)
    perm_t[...] = (packed_place(c_io) == r_io).astype(BF16)

    tok = tok_ref.shape[0]
    slots = CHUNKS * GROUP
    sub = lax.broadcasted_iota(jnp.int32, (tok, tok), 0)
    lane = lax.broadcasted_iota(jnp.int32, (tok, tok), 1)
    same = sub == lane

    def as_row(col, zero):
        return jnp.sum(jnp.where(same, jnp.broadcast_to(col, (tok, tok)), zero), axis=0, keepdims=True)

    def as_col(row, zero):
        return jnp.sum(jnp.where(same, jnp.broadcast_to(row, (tok, tok)), zero), axis=1, keepdims=True)

    cols = [routes_ref[:, k : k + 1] for k in range(2)]
    slot_iota = lax.broadcasted_iota(jnp.int32, (slots, tok), 0)
    place_iota = lax.broadcasted_iota(jnp.int32, (tok, slots), 1)
    dispatch = jnp.zeros((slots, tok), F32)
    comb = jnp.zeros((tok, slots), F32)
    for k in range(2):
        e = as_row(cols[k], 0)
        rank = jnp.sum(
            jnp.where(sub < lane, (cols[0] == e).astype(jnp.int32) + (cols[1] == e).astype(jnp.int32), 0),
            axis=0,
            keepdims=True,
        )
        ez, ey, ec = e >> 3, (e >> 1) & (NY - 1), e & (NC - 1)
        offset = ((ey + NY - y) & (NY - 1)) * BLOCKS + ((ez + NZ - z) & (NZ - 1)) * NC + ((ec + c) & (NC - 1))
        slot = offset * CAP + rank
        dispatch = dispatch + (slot_iota == slot).astype(F32)
        comb = comb + jnp.where(place_iota == as_col(slot, 0), rw_ref[:, k : k + 1], 0.0)
    high = comb.astype(BF16)
    comb_ref[:tok] = high
    comb_ref[tok:] = (comb - high.astype(F32)).astype(BF16)
    widened = tok_ref[...].astype(F32)
    normed = (
        widened * lax.rsqrt(jnp.mean(widened * widened, axis=1, keepdims=True) + 1e-06) * ng_ref[...]
    ).astype(BF16)
    ordered = jnp.dot(dispatch.astype(BF16), normed, preferred_element_type=F32).astype(BF16)
    width = ordered.shape[1] // QUARTERS

    def pack(block):
        tall = jnp.concatenate([block[:, kq * width : (kq + 1) * width] for kq in range(QUARTERS)], axis=0)
        turned = jnp.dot(perm_t[...], tall, preferred_element_type=F32).astype(BF16)
        return turned.reshape(BLOCKS, QUARTERS * CAP, width)

    for g in range(CHUNKS):
        outbound[g] = pack(ordered[g * GROUP : (g + 1) * GROUP])
    heads = q_in.shape[1] // 128
    map_lane = lax.broadcasted_iota(jnp.int32, (q_in.shape[0], 128), 1) < 64
    for h in range(heads):
        scaled = (q_in[:, h * 128 : (h + 1) * 128].astype(F32) * 0.125)
        q_ref[h] = jnp.where(map_lane, scaled, 0.0).astype(BF16)
        q_ref[heads + h] = jnp.where(map_lane, 0.0, scaled).astype(BF16)

    for ref, buf, j in kv:
        pltpu.make_async_copy(ref, buf.at[z, y, c], kv_own.at[j]).wait()
    with jax.named_scope("barrier"):
        pl.semaphore_wait(barrier, CHUNKS * BLOCKS - 1 + NX - 1)

    z_up = {"ep_0": lax.rem(z + 1, NZ)}
    z_down = {"ep_0": lax.rem(z + NZ - 1, NZ)}

    def zb(k):
        return lax.rem(z + NZ + k, NZ)

    def z_copies(k):
        ups = [rcopy(b.at[zb(1 - k), y, c], b.at[zb(1 - k), y, c], z_send.at[k - 1, 0, j], z_recv.at[k - 1, 0, j], z_up)
               for _, b, j in kv if k < 4 or j == 0]
        downs = [rcopy(b.at[zb(k - 1), y, c], b.at[zb(k - 1), y, c], z_send.at[k - 1, 1, j], z_recv.at[k - 1, 1, j], z_down)
                 for _, b, j in kv if k < 4 or j == 1]
        return ups + downs

    def z_blocks(k):
        return (0,) if k == 0 else (4,) if k == 4 else (-k, k)

    def y_copies(k):
        out = []
        for n, dz in enumerate(z_blocks(k)):
            for _, b, j in kv:
                ref = b.at[zb(dz), y, c]
                for d, dev in enumerate((y_up, y_down)):
                    out.append(rcopy(ref, ref, y_send.at[k, n, d, j], y_recv.at[k, n, d, j], dev))
        return out

    def hop_copies(k):
        out = []
        for n, dz in enumerate(z_blocks(k)):
            lo = kbuf.at[zb(dz), ym1, c]
            out.append(rcopy(lo, lo, h_send.at[k, n, 0], h_recv.at[k, n, 0], y_up))
            hi = vbuf.at[zb(dz), yp1, c]
            out.append(rcopy(hi, hi, h_send.at[k, n, 1], h_recv.at[k, n, 1], y_down))
        return out

    def core_copies():
        return [rcopy(b.at[:, :, c], b.at[:, :, c], c_send.at[j], c_recv.at[j], partner) for _, b, j in kv]

    def start(copies):
        for copy in copies:
            copy.start()

    def landed(copies):
        for copy in copies:
            copy.wait_recv()

    def send_rows(g):
        for dz in dz_order():
            for dc in range(NC):
                i = dz * NC + dc
                if isinstance(g, int) and g == 0 and i == 0:
                    pltpu.make_async_copy(outbound.at[0, 0], arr.at[0, 0], a_recv.at[0]).start()
                    continue
                dev = {
                    "ep_0": lax.rem(z + dz, NZ),
                    "ep_1": lax.rem(y + g, NY),
                    "ep_2": (1 - c) if dc else c,
                }
                rcopy(outbound.at[g, i], arr.at[g, i], a_send.at[0], a_recv.at[g], dev).start()

    start(z_copies(1))
    start(y_copies(0))
    send_rows(0)
    send_rows(1)
    with jax.named_scope("kv_1"):
        landed(z_copies(1))
    start(z_copies(2))
    start(y_copies(1))
    send_rows(2)

    def relayout_in(src, g, store):
        tile = src[g].reshape(size, width)
        turned = jnp.dot(perm[...], tile, preferred_element_type=F32).astype(BF16)
        for kq in range(QUARTERS):
            store(kq, turned[kq * GROUP : (kq + 1) * GROUP])

    def gather_first(g):
        pltpu.make_async_copy(arr.at[g], arr.at[g], a_recv.at[g]).wait()

        def store(kq, value):
            xb[g, 0, :, kq * width : (kq + 1) * width] = value

        relayout_in(arr, g, store)
        rcopy(xb.at[g, 0], xb.at[g, 1], x_send.at[0, g], x_recv.at[0, g], right).start()
        rcopy(xb.at[g, 0], xb.at[g, 2], x_send.at[1, g], x_recv.at[1, g], left).start()

    top, low = pl.ds(0, GROUP // 2), pl.ds(GROUP // 2, GROUP // 2)

    def gather_second(g):
        rcopy(xb.at[g, 0], xb.at[g, 1], x_send.at[0, g], x_recv.at[0, g], right).wait_recv()
        rcopy(xb.at[g, 1, top], xb.at[g, 3, top], f_send.at[0, g], f_recv.at[0, g], right).start()
        rcopy(xb.at[g, 0], xb.at[g, 2], x_send.at[1, g], x_recv.at[1, g], left).wait_recv()
        rcopy(xb.at[g, 2, low], xb.at[g, 3, low], f_send.at[1, g], f_recv.at[1, g], left).start()

    ffe = gw.shape[1]
    model = gw.shape[0]
    rows = NX * GROUP

    def experts(g):
        rcopy(xb.at[g, 1, top], xb.at[g, 3, top], f_send.at[0, g], f_recv.at[0, g], right).wait_recv()
        rcopy(xb.at[g, 2, low], xb.at[g, 3, low], f_send.at[1, g], f_recv.at[1, g], left).wait_recv()

        @pl.when(g == 0)
        def _():
            for copy in weights[:3]:
                copy.wait()

        inputs = xb[g].reshape(rows, model)
        for n in range(0, ffe, 256):
            w = min(256, ffe - n)
            gate = jnp.dot(inputs, gw[:, n : n + w], preferred_element_type=F32)
            up = jnp.dot(inputs, uw[:, n : n + w], preferred_element_type=F32)
            hid[:, n : n + w] = (gate / (1.0 + jnp.exp(-gate)) * up).astype(BF16)
        hidden = hid[...]
        for n in range(0, model, 256):
            part[g, :, :, n : n + 256] = (
                jnp.dot(hidden, dw[:, n : n + 256], preferred_element_type=F32).astype(BF16).reshape(NX, GROUP, 256)
            )
        rcopy(part.at[g, 3, top], opp.at[g, 0], s1_send.at[0, g], s1_recv.at[0, g], right).start()
        rcopy(part.at[g, 3, low], opp.at[g, 1], s1_send.at[1, g], s1_recv.at[1, g], left).start()
        rcopy(part.at[g, 2, low], fin.at[g, 0, low], s2_send.at[0, g], fin_recv.at[0, g], right).start()
        rcopy(part.at[g, 1, top], fin.at[g, 1, top], s2_send.at[1, g], fin_recv.at[1, g], left).start()

    def sum_second(g):
        rcopy(part.at[g, 3, top], opp.at[g, 0], s1_send.at[0, g], s1_recv.at[0, g], right).wait_recv()
        part[g, 2, : GROUP // 2] = (part[g, 2, : GROUP // 2].astype(F32) + opp[g, 0].astype(F32)).astype(BF16)
        rcopy(part.at[g, 2, top], fin.at[g, 0, top], s2_send.at[2, g], fin_recv.at[2, g], right).start()
        rcopy(part.at[g, 3, low], opp.at[g, 1], s1_send.at[1, g], s1_recv.at[1, g], left).wait_recv()
        part[g, 1, GROUP // 2 :] = (part[g, 1, GROUP // 2 :].astype(F32) + opp[g, 1].astype(F32)).astype(BF16)
        rcopy(part.at[g, 1, low], fin.at[g, 1, low], s2_send.at[3, g], fin_recv.at[3, g], left).start()

    def sum_last(g):
        rcopy(part.at[g, 2, low], fin.at[g, 0, low], s2_send.at[0, g], fin_recv.at[0, g], right).wait_recv()
        rcopy(part.at[g, 1, top], fin.at[g, 1, top], s2_send.at[1, g], fin_recv.at[1, g], left).wait_recv()
        rcopy(part.at[g, 2, top], fin.at[g, 0, top], s2_send.at[2, g], fin_recv.at[2, g], right).wait_recv()
        rcopy(part.at[g, 1, low], fin.at[g, 1, low], s2_send.at[3, g], fin_recv.at[3, g], left).wait_recv()
        total = (part[g, 0].astype(F32) + fin[g, 0].astype(F32) + fin[g, 1].astype(F32)).astype(BF16)
        back[g] = pack(total)
        for dz in dz_order():
            for dc in range(NC):
                i = dz * NC + dc

                def go():
                    dev = {
                        "ep_0": lax.rem(z + NZ - dz, NZ),
                        "ep_1": lax.rem(y + NY - g, NY),
                        "ep_2": (1 - c) if dc else c,
                    }
                    rcopy(back.at[g, i], ret.at[g, i], b_send.at[0], r_recv.at[g], dev).start()

                if i == 0:
                    pl.when(g > 0)(go)

                    @pl.when(g == 0)
                    def _():
                        pltpu.make_async_copy(back.at[0, 0], ret.at[0, 0], r_recv.at[0]).start()

                else:
                    go()

    ta = q_ref.shape[1]
    span = NY * NC * ta

    def attend_plane(t, masked):
        kc = kbuf[t].reshape(span, kbuf.shape[-1])
        vc = jnp.concatenate([vbuf[t].reshape(span, vbuf.shape[-1]), jnp.ones((span, 128), BF16)], axis=1)
        for r in range(2 * heads):
            s = lax.dot_general(q_ref[r], kc, (((1,), (1,)), ((), ())), preferred_element_type=F32)
            if masked:
                kpos = t * span + lax.broadcasted_iota(jnp.int32, s.shape, 1)
                qpos = me * ta + lax.broadcasted_iota(jnp.int32, s.shape, 0)
                s = jnp.where(kpos <= qpos, s, NEG_LARGE)
            old = m_ref[r][:, :1]
            new = jnp.maximum(old, jnp.max(s, axis=1, keepdims=True))
            p = jnp.exp(s - new)
            scale = jnp.exp(old - new)
            m_ref[r] = jnp.broadcast_to(new, m_ref.shape[1:])
            acc_ref[r] = acc_ref[r] * scale + jnp.dot(p.astype(BF16), vc, preferred_element_type=F32)

    def attend_some(first, end):
        def step(t, carry):
            attend_plane(t, False)
            return carry

        lax.fori_loop(first, jnp.maximum(first, jnp.minimum(end, z)), step, 0)

    def attend_first():
        with jax.named_scope("wait_kv"):
            landed(core_copies())
        m_ref[...] = jnp.full(m_ref.shape, NEG_LARGE, F32)
        acc_ref[...] = jnp.zeros(acc_ref.shape, F32)
        attend_some(0, 3)

    def attend_last():
        attend_plane(z, True)
        for h in range(heads):
            one, two = acc_ref[h], acc_ref[heads + h]
            blended = one[:, :128] / one[:, 128:] - mix_ref[h] * (two[:, :128] / two[:, 128:])
            normed = (
                blended * lax.rsqrt(jnp.mean(blended * blended, axis=1, keepdims=True) + 1e-05) * gain_ref[...]
            ).astype(BF16)
            att_ref[:, :, h * 128 : (h + 1) * 128] = normed.reshape(NX, ta // NX, 128)
        weights[3].wait()
        for r in range(NX):
            j = lax.rem(x + r, NX)
            ap[r] = jnp.dot(att_ref[j], ow_ref[...], preferred_element_type=F32).astype(BF16)
            if r:
                rcopy(ap.at[r], ar.at[r - 1], at_send.at[r - 1], at_recv.at[r - 1], {"tp": j}).start()

    def main(s, carry):
        @pl.when((s >= 4) & (s < CHUNKS + 4))
        def _():
            with jax.named_scope("sum_last"):
                sum_last(s - 4)

        @pl.when((s >= 3) & (s < CHUNKS + 3))
        def _():
            with jax.named_scope("sum_second"):
                sum_second(s - 3)

        @pl.when(s < CHUNKS)
        def _():
            with jax.named_scope("gather_first"):
                gather_first(s)

        @pl.when((s >= 1) & (s < CHUNKS + 1))
        def _():
            with jax.named_scope("gather_second"):
                gather_second(s - 1)

        @pl.when(s == 0)
        def _():
            with jax.named_scope("kv_2"):
                landed(z_copies(2))
                start(z_copies(3))
                start(y_copies(2))
                send_rows(3)
                landed(y_copies(0))
                start(hop_copies(0))

        @pl.when(s == 1)
        def _():
            with jax.named_scope("kv_3"):
                landed(z_copies(3))
                start(z_copies(4))
                start(y_copies(3))
                landed(y_copies(1))
                start(hop_copies(1))

        @pl.when(s == 2)
        def _():
            with jax.named_scope("kv_4"):
                landed(z_copies(4))
                start(y_copies(4))
                landed(y_copies(2))
                start(hop_copies(2))

        @pl.when(s == 3)
        def _():
            with jax.named_scope("kv_5"):
                for k in (3, 4):
                    landed(y_copies(k))
                    start(hop_copies(k))

        @pl.when(s == 4)
        def _():
            with jax.named_scope("kv_6"):
                for k in range(5):
                    landed(hop_copies(k))
                start(core_copies())

        @pl.when((s >= 2) & (s < CHUNKS + 2))
        def _():
            with jax.named_scope("experts"):
                experts(s - 2)

        @pl.when(s == CHUNKS)
        def _():
            with jax.named_scope("attend_1"):
                attend_first()

        @pl.when(s == CHUNKS + 1)
        def _():
            with jax.named_scope("attend_2"):
                attend_some(3, 5)

        @pl.when(s == CHUNKS + 2)
        def _():
            with jax.named_scope("attend_3"):
                attend_some(5, NZ)
                attend_last()

        return carry

    lax.fori_loop(0, CHUNKS + 4, main, 0)

    for r in range(1, NX):
        rcopy(ap.at[r], ar.at[r - 1], at_send.at[r - 1], at_recv.at[r - 1], right).wait_recv()
    total = ap[0].astype(F32)
    for r in range(1, NX):
        total = total + ar[r - 1].astype(F32)
    attn_o[...] = total.astype(BF16)

    def collect(g, carry):
        with jax.named_scope("wait_ret"):
            pltpu.make_async_copy(ret.at[g], ret.at[g], r_recv.at[g]).wait()

        def store(kq, value):
            rows_ref[pl.ds(pl.multiple_of(g * GROUP, GROUP), GROUP), kq * width : (kq + 1) * width] = value

        relayout_in(ret, g, store)
        return carry

    lax.fori_loop(0, CHUNKS, collect, 0)
    tokens = tok
    for kq in range(QUARTERS):
        both = jnp.dot(comb_ref[...], rows_ref[:, kq * width : (kq + 1) * width], preferred_element_type=F32)
        moe_o[:, kq * width : (kq + 1) * width] = (both[:tokens] + both[tokens:]).astype(BF16)

    for g in range(CHUNKS):
        for copy in (
            rcopy(xb.at[g, 0], xb.at[g, 1], x_send.at[0, g], x_recv.at[0, g], right),
            rcopy(xb.at[g, 0], xb.at[g, 2], x_send.at[1, g], x_recv.at[1, g], left),
            rcopy(xb.at[g, 1, top], xb.at[g, 3, top], f_send.at[0, g], f_recv.at[0, g], right),
            rcopy(xb.at[g, 2, low], xb.at[g, 3, low], f_send.at[1, g], f_recv.at[1, g], left),
            rcopy(part.at[g, 3, top], opp.at[g, 0], s1_send.at[0, g], s1_recv.at[0, g], right),
            rcopy(part.at[g, 3, low], opp.at[g, 1], s1_send.at[1, g], s1_recv.at[1, g], left),
            rcopy(part.at[g, 2, low], fin.at[g, 0, low], s2_send.at[0, g], fin_recv.at[0, g], right),
            rcopy(part.at[g, 1, top], fin.at[g, 1, top], s2_send.at[1, g], fin_recv.at[1, g], left),
            rcopy(part.at[g, 2, top], fin.at[g, 0, top], s2_send.at[2, g], fin_recv.at[2, g], right),
            rcopy(part.at[g, 1, low], fin.at[g, 1, low], s2_send.at[3, g], fin_recv.at[3, g], left),
        ):
            copy.wait_send()
    for r in range(1, NX):
        rcopy(ap.at[r], ar.at[r - 1], at_send.at[r - 1], at_recv.at[r - 1], right).wait_send()
    for k in range(1, 5):
        for copy in z_copies(k):
            copy.wait_send()
    for k in range(5):
        for copy in y_copies(k) + hop_copies(k):
            copy.wait_send()
    for copy in core_copies():
        copy.wait_send()
    for sem, buf in ((a_send, outbound), (b_send, back)):
        for g in range(CHUNKS):
            blocks = buf.at[g, pl.ds(1, BLOCKS - 1)] if g == 0 else buf.at[g]
            rcopy(blocks, blocks, sem.at[0], r_recv.at[g], right).wait_send()


def body(
    queries,
    keys,
    values,
    mix_scale,
    head_gain,
    out_weight,
    moe_input,
    norm_gain,
    routes,
    route_weights,
    gate_weight,
    up_weight,
    down_weight,
):
    ta, heads, qd = queries.shape
    tok, model = moe_input.shape
    ffe = gate_weight.shape[2]
    vd = values.shape[2]
    width = model // QUARTERS
    slots = CHUNKS * GROUP
    vmem = pl.BlockSpec(memory_space=pltpu.VMEM)
    hbm = pl.BlockSpec(memory_space=pl.ANY)
    dma = pltpu.SemaphoreType.DMA
    size = BLOCKS * QUARTERS * CAP
    attn_out, moe_out = pl.pallas_call(
        kernel,
        out_shape=(
            jax.ShapeDtypeStruct((ta // NX, model), BF16),
            jax.ShapeDtypeStruct((tok, model), BF16),
        ),
        in_specs=[vmem] * 5 + [vmem] * 2 + [pl.BlockSpec(memory_space=pltpu.SMEM), vmem] + [hbm] * 4,
        out_specs=(vmem, vmem),
        scratch_shapes=[
            pltpu.VMEM((model, ffe), BF16),
            pltpu.VMEM((model, ffe), BF16),
            pltpu.VMEM((ffe, model), BF16),
            pltpu.VMEM((heads * vd, model), BF16),
            pltpu.VMEM((CHUNKS, BLOCKS, QUARTERS * CAP, width), BF16),
            pltpu.VMEM((2 * heads, ta, qd), BF16),
            pltpu.VMEM((2 * tok, slots), BF16),
            pltpu.VMEM((NZ, NY, NC, ta, qd), BF16),
            pltpu.VMEM((NZ, NY, NC, ta, vd), BF16),
            pltpu.VMEM((size, size), BF16),
            pltpu.VMEM((size, size), BF16),
            pltpu.VMEM((CHUNKS, BLOCKS, QUARTERS * CAP, width), BF16),
            pltpu.VMEM((CHUNKS, NX, GROUP, model), BF16),
            pltpu.VMEM((NX * GROUP, ffe), BF16),
            pltpu.VMEM((CHUNKS, NX, GROUP, model), BF16),
            pltpu.VMEM((CHUNKS, 2, GROUP // 2, model), BF16),
            pltpu.VMEM((CHUNKS, 2, GROUP, model), BF16),
            pltpu.VMEM((CHUNKS, BLOCKS, QUARTERS * CAP, width), BF16),
            pltpu.VMEM((CHUNKS, BLOCKS, QUARTERS * CAP, width), BF16),
            pltpu.VMEM((slots, model), BF16),
            pltpu.VMEM((2 * heads, ta, 128), F32),
            pltpu.VMEM((2 * heads, ta, 2 * vd), F32),
            pltpu.VMEM((NX, ta // NX, heads * vd), BF16),
            pltpu.VMEM((NX, ta // NX, model), BF16),
            pltpu.VMEM((NX - 1, ta // NX, model), BF16),
            dma((4,)),
            dma((2,)),
            dma((4, 2, 2)),
            dma((4, 2, 2)),
            dma((5, 2, 2, 2)),
            dma((5, 2, 2, 2)),
            dma((5, 2, 2)),
            dma((5, 2, 2)),
            dma((2,)),
            dma((2,)),
            dma((1,)),
            dma((CHUNKS,)),
            dma((2, CHUNKS)),
            dma((2, CHUNKS)),
            dma((2, CHUNKS)),
            dma((2, CHUNKS)),
            dma((2, CHUNKS)),
            dma((2, CHUNKS)),
            dma((4, CHUNKS)),
            dma((4, CHUNKS)),
            dma((1,)),
            dma((CHUNKS,)),
            dma((NX - 1,)),
            dma((NX - 1,)),
        ],
        compiler_params=pltpu.CompilerParams(collective_id=0, has_side_effects=True, vmem_limit_bytes=62 * 1024 * 1024),
    )(
        moe_input,
        norm_gain.reshape(1, model),
        routes,
        route_weights,
        queries.reshape(ta, heads * qd),
        keys.reshape(ta, qd),
        values.reshape(ta, vd),
        mix_scale,
        head_gain.reshape(1, vd),
        out_weight.reshape(heads * vd, model),
        gate_weight[0],
        up_weight[0],
        down_weight[0],
    )
    return (attn_out, moe_out)


def solution(mesh):
    split = Mesh(mesh.devices.reshape(NZ, NY, NC, NX), EP_TP)
    placed = (
        P(EP, "tp", None),
        P(EP, "tp", None),
        P(EP, "tp", None),
        P("tp"),
        P(),
        P("tp", None, None),
        P(EP_TP, None),
        P(),
        P(EP_TP, None),
        P(EP_TP, None),
        P(EP, None, "tp"),
        P(EP, None, "tp"),
        P(EP, "tp", None),
    )
    return jax.shard_map(
        body,
        mesh=split,
        in_specs=placed,
        out_specs=(P(EP_TP, None), P(EP_TP, None)),
        check_vma=False,
    )
```

```python
import functools

import jax
import jax.numpy as jnp
from jax import lax
from jax.experimental import pallas as pl
from jax.experimental.pallas import tpu as pltpu
from jax.sharding import Mesh
from jax.sharding import PartitionSpec as P

EP = ("ep_0", "ep_1", "ep_2")
EP_TP = ("ep_0", "ep_1", "ep_2", "tp")
MESH = pl.DeviceIdType.MESH

NZ, NY, NC, NX = 8, 4, 2, 4
CHUNKS = 4
BLOCKS = NZ * NY * NC // CHUNKS
CAP = 4
QUARTERS = 4
GROUP = BLOCKS * CAP
NEG_LARGE = -1e30
F32 = jnp.float32
BF16 = jnp.bfloat16


def offsets():
    out = [(0, dy, dc) for dy in range(NY) for dc in range(NC)]
    for k in (1, 2, 3):
        out += [(dz, dy, dc) for dc in range(NC) for dy in range(NY) for dz in (k, NZ - k)]
    return out + [(NZ // 2, dy, dc) for dy in range(NY) for dc in range(NC)]


OFFSETS = offsets()


def place_of(dz, dy, dc):
    k = jnp.minimum(dz, NZ - dz)
    ends = dy * NC + dc
    between = 16 * k - 8 + dc * 8 + dy * 2 + (dz > NZ // 2).astype(jnp.int32)
    return jnp.where(k == 0, ends, jnp.where(k == NZ // 2, 56 + ends, between))


def kernel(
    tok_ref,
    ng_ref,
    routes_ref,
    rw_ref,
    q_in,
    k_ref,
    v_ref,
    mix_ref,
    gain_ref,
    ow_hbm,
    gw_hbm,
    uw_hbm,
    dw_hbm,
    attn_o,
    moe_o,
    gw,
    uw,
    dw,
    ow_ref,
    outbound,
    q_ref,
    comb_ref,
    kbuf,
    vbuf,
    perm,
    perm_t,
    arr,
    xb,
    hid,
    part,
    opp,
    fin,
    back,
    ret,
    rows_ref,
    m_ref,
    acc_ref,
    att_ref,
    ap,
    ao,
    ar,
    w_sem,
    kv_own,
    z_send,
    z_recv,
    y_send,
    y_recv,
    h_send,
    h_recv,
    c_send,
    c_recv,
    a_send,
    a_recv,
    x_send,
    x_recv,
    f_send,
    f_recv,
    s1_send,
    s1_recv,
    s2_send,
    fin_recv,
    b_send,
    r_recv,
    at_send,
    at_recv,
):
    z = lax.axis_index("ep_0")
    y = lax.axis_index("ep_1")
    c = lax.axis_index("ep_2")
    x = lax.axis_index("tp")
    me = z * (NY * NC) + y * NC + c
    right = {"tp": lax.rem(x + 1, NX)}
    left = {"tp": lax.rem(x + NX - 1, NX)}
    y_up = {"ep_1": lax.rem(y + 1, NY)}
    y_down = {"ep_1": lax.rem(y + NY - 1, NY)}
    ym1 = lax.rem(y + NY - 1, NY)
    yp1 = lax.rem(y + 1, NY)
    partner = {"ep_2": 1 - c}

    def rcopy(src, dst, ssem, rsem, dev):
        return pltpu.make_async_remote_copy(
            src_ref=src, dst_ref=dst, send_sem=ssem, recv_sem=rsem, device_id=dev, device_id_type=MESH
        )

    barrier = pltpu.get_barrier_semaphore()

    def at_offset(i):
        dz, dy, dc = OFFSETS[i]
        return {"ep_0": lax.rem(z + dz, NZ), "ep_1": lax.rem(y + dy, NY), "ep_2": (1 - c) if dc else c}

    def from_offset(i):
        dz, dy, dc = OFFSETS[i]
        return {"ep_0": lax.rem(z + NZ - dz, NZ), "ep_1": lax.rem(y + NY - dy, NY), "ep_2": (1 - c) if dc else c}

    for i in range(CHUNKS * BLOCKS - 1, 0, -1):
        pl.semaphore_signal(barrier, inc=1, device_id=at_offset(i), device_id_type=MESH)
    for r in range(1, NX):
        pl.semaphore_signal(barrier, inc=1, device_id={"tp": lax.rem(x + r, NX)}, device_id_type=MESH)

    kv = ((k_ref, kbuf, 0), (v_ref, vbuf, 1))
    for ref, buf, j in kv:
        pltpu.make_async_copy(ref, buf.at[z, y, c], kv_own.at[j]).start()
    weights = [
        pltpu.make_async_copy(s, d, w_sem.at[i])
        for i, (s, d) in enumerate(((gw_hbm, gw), (uw_hbm, uw), (dw_hbm, dw), (ow_hbm, ow_ref)))
    ]
    for copy in weights:
        copy.start()

    size = BLOCKS * QUARTERS * CAP
    r_io = lax.broadcasted_iota(jnp.int32, (size, size), 0)
    c_io = lax.broadcasted_iota(jnp.int32, (size, size), 1)

    def packed_place(r):
        return (r % GROUP) // CAP * (QUARTERS * CAP) + r // GROUP * CAP + r % CAP

    perm[...] = (packed_place(r_io) == c_io).astype(BF16)
    perm_t[...] = (packed_place(c_io) == r_io).astype(BF16)

    tok = tok_ref.shape[0]
    slots = CHUNKS * GROUP
    sub = lax.broadcasted_iota(jnp.int32, (tok, tok), 0)
    lane = lax.broadcasted_iota(jnp.int32, (tok, tok), 1)
    same = sub == lane

    def as_col(row, zero):
        return jnp.sum(jnp.where(same, jnp.broadcast_to(row, (tok, tok)), zero), axis=1, keepdims=True)

    named = [routes_ref[k : k + 1, :] for k in range(2)]
    cols = [as_col(row, 0) for row in named]
    slot_iota = lax.broadcasted_iota(jnp.int32, (slots, tok), 0)
    place_iota = lax.broadcasted_iota(jnp.int32, (tok, slots), 1)
    dispatch = jnp.zeros((slots, tok), F32)
    comb = jnp.zeros((tok, slots), F32)
    for k in range(2):
        e = named[k]
        rank = jnp.sum(
            jnp.where(sub < lane, (cols[0] == e).astype(jnp.int32) + (cols[1] == e).astype(jnp.int32), 0),
            axis=0,
            keepdims=True,
        )
        ez, ey, ec = e >> 3, (e >> 1) & (NY - 1), e & (NC - 1)
        offset = place_of((ez + NZ - z) & (NZ - 1), (ey + NY - y) & (NY - 1), (ec + c) & (NC - 1))
        slot = offset * CAP + rank
        dispatch = dispatch + (slot_iota == slot).astype(F32)
        comb = comb + jnp.where(place_iota == as_col(slot, 0), as_col(rw_ref[k : k + 1, :], 0.0), 0.0)
    high = comb.astype(BF16)
    comb_ref[:tok] = high
    comb_ref[tok:] = (comb - high.astype(F32)).astype(BF16)
    widened = tok_ref[...].astype(F32)
    normed = (
        widened * lax.rsqrt(jnp.mean(widened * widened, axis=1, keepdims=True) + 1e-06) * ng_ref[...]
    ).astype(BF16)
    ordered = jnp.dot(dispatch.astype(BF16), normed, preferred_element_type=F32).astype(BF16)
    width = ordered.shape[1] // QUARTERS

    def pack(block):
        tall = jnp.concatenate([block[:, kq * width : (kq + 1) * width] for kq in range(QUARTERS)], axis=0)
        turned = jnp.dot(perm_t[...], tall, preferred_element_type=F32).astype(BF16)
        return turned.reshape(BLOCKS, QUARTERS * CAP, width)

    for g in range(CHUNKS):
        outbound[g] = pack(ordered[g * GROUP : (g + 1) * GROUP])
    for ref, buf, j in kv:
        pltpu.make_async_copy(ref, buf.at[z, y, c], kv_own.at[j]).wait()
    with jax.named_scope("barrier"):
        pl.semaphore_wait(barrier, CHUNKS * BLOCKS - 1 + NX - 1)

    z_up = {"ep_0": lax.rem(z + 1, NZ)}
    z_down = {"ep_0": lax.rem(z + NZ - 1, NZ)}

    def zb(k):
        return lax.rem(z + NZ + k, NZ)

    def z_copies(k):
        ups = [rcopy(b.at[zb(1 - k), y, c], b.at[zb(1 - k), y, c], z_send.at[k - 1, 0, j], z_recv.at[k - 1, 0, j], z_up)
               for _, b, j in kv if k < 4 or j == 0]
        downs = [rcopy(b.at[zb(k - 1), y, c], b.at[zb(k - 1), y, c], z_send.at[k - 1, 1, j], z_recv.at[k - 1, 1, j], z_down)
                 for _, b, j in kv if k < 4 or j == 1]
        return ups + downs

    def z_blocks(k):
        return (0,) if k == 0 else (4,) if k == 4 else (-k, k)

    def y_copies(k):
        out = []
        for n, dz in enumerate(z_blocks(k)):
            for _, b, j in kv:
                ref = b.at[zb(dz), y, c]
                for d, dev in enumerate((y_up, y_down)):
                    out.append(rcopy(ref, ref, y_send.at[k, n, d, j], y_recv.at[k, n, d, j], dev))
        return out

    def hop_copies(k):
        out = []
        for n, dz in enumerate(z_blocks(k)):
            lo = kbuf.at[zb(dz), ym1, c]
            out.append(rcopy(lo, lo, h_send.at[k, n, 0], h_recv.at[k, n, 0], y_up))
            hi = vbuf.at[zb(dz), yp1, c]
            out.append(rcopy(hi, hi, h_send.at[k, n, 1], h_recv.at[k, n, 1], y_down))
        return out

    def core_copies():
        return [rcopy(b.at[:, :, c], b.at[:, :, c], c_send.at[j], c_recv.at[j], partner) for _, b, j in kv]

    def start(copies):
        for copy in copies:
            copy.start()

    def landed(copies):
        for copy in copies:
            copy.wait_recv()

    def send_rows(g):
        for i in range(BLOCKS):
            if g == 0 and i == 0:
                pltpu.make_async_copy(outbound.at[0, 0], arr.at[0, 0], a_recv.at[0]).start()
            else:
                rcopy(outbound.at[g, i], arr.at[g, i], a_send.at[0], a_recv.at[g], at_offset(g * BLOCKS + i)).start()

    def relayout_in(src, g, store):
        tile = src[g].reshape(size, width)
        turned = jnp.dot(perm[...], tile, preferred_element_type=F32).astype(BF16)
        for kq in range(QUARTERS):
            store(kq, turned[kq * GROUP : (kq + 1) * GROUP])

    def gather_first(g):
        pltpu.make_async_copy(arr.at[g], arr.at[g], a_recv.at[g]).wait()

        def store(kq, value):
            xb[g, 0, :, kq * width : (kq + 1) * width] = value

        relayout_in(arr, g, store)
        rcopy(xb.at[g, 0], xb.at[g, 1], x_send.at[0, g], x_recv.at[0, g], right).start()
        rcopy(xb.at[g, 0], xb.at[g, 2], x_send.at[1, g], x_recv.at[1, g], left).start()

    top, low = pl.ds(0, GROUP // 2), pl.ds(GROUP // 2, GROUP // 2)

    def gather_second(g):
        rcopy(xb.at[g, 0], xb.at[g, 1], x_send.at[0, g], x_recv.at[0, g], right).wait_recv()
        rcopy(xb.at[g, 1, top], xb.at[g, 3, top], f_send.at[0, g], f_recv.at[0, g], right).start()
        rcopy(xb.at[g, 0], xb.at[g, 2], x_send.at[1, g], x_recv.at[1, g], left).wait_recv()
        rcopy(xb.at[g, 2, low], xb.at[g, 3, low], f_send.at[1, g], f_recv.at[1, g], left).start()

    ffe = gw.shape[1]
    model = gw.shape[0]
    rows = NX * GROUP

    def experts(g):
        rcopy(xb.at[g, 1, top], xb.at[g, 3, top], f_send.at[0, g], f_recv.at[0, g], right).wait_recv()
        rcopy(xb.at[g, 2, low], xb.at[g, 3, low], f_send.at[1, g], f_recv.at[1, g], left).wait_recv()

        @pl.when(g == 0)
        def _():
            for copy in weights[:3]:
                copy.wait()

        inputs = xb[g].reshape(rows, model)
        for n in range(0, ffe, 256):
            w = min(256, ffe - n)
            gate = jnp.dot(inputs, gw[:, n : n + w], preferred_element_type=F32)
            up = jnp.dot(inputs, uw[:, n : n + w], preferred_element_type=F32)
            hid[:, n : n + w] = (gate / (1.0 + jnp.exp(-gate)) * up).astype(BF16)
        hidden = hid[...]
        for n in range(0, model, 256):
            part[g, :, :, n : n + 256] = (
                jnp.dot(hidden, dw[:, n : n + 256], preferred_element_type=F32).astype(BF16).reshape(NX, GROUP, 256)
            )

    def sum_first(g):
        rcopy(part.at[g, 3, top], opp.at[g, 0], s1_send.at[0, g], s1_recv.at[0, g], right).start()
        rcopy(part.at[g, 3, low], opp.at[g, 1], s1_send.at[1, g], s1_recv.at[1, g], left).start()
        rcopy(part.at[g, 2, low], fin.at[g, 0, low], s2_send.at[0, g], fin_recv.at[0, g], right).start()
        rcopy(part.at[g, 1, top], fin.at[g, 1, top], s2_send.at[1, g], fin_recv.at[1, g], left).start()

    def sum_second(g):
        rcopy(part.at[g, 3, top], opp.at[g, 0], s1_send.at[0, g], s1_recv.at[0, g], right).wait_recv()
        part[g, 2, : GROUP // 2] = (part[g, 2, : GROUP // 2].astype(F32) + opp[g, 0].astype(F32)).astype(BF16)
        rcopy(part.at[g, 2, top], fin.at[g, 0, top], s2_send.at[2, g], fin_recv.at[2, g], right).start()
        rcopy(part.at[g, 3, low], opp.at[g, 1], s1_send.at[1, g], s1_recv.at[1, g], left).wait_recv()
        part[g, 1, GROUP // 2 :] = (part[g, 1, GROUP // 2 :].astype(F32) + opp[g, 1].astype(F32)).astype(BF16)
        rcopy(part.at[g, 1, low], fin.at[g, 1, low], s2_send.at[3, g], fin_recv.at[3, g], left).start()

    def sum_last(g):
        rcopy(part.at[g, 2, low], fin.at[g, 0, low], s2_send.at[0, g], fin_recv.at[0, g], right).wait_recv()
        rcopy(part.at[g, 1, top], fin.at[g, 1, top], s2_send.at[1, g], fin_recv.at[1, g], left).wait_recv()
        rcopy(part.at[g, 2, top], fin.at[g, 0, top], s2_send.at[2, g], fin_recv.at[2, g], right).wait_recv()
        rcopy(part.at[g, 1, low], fin.at[g, 1, low], s2_send.at[3, g], fin_recv.at[3, g], left).wait_recv()
        total = (part[g, 0].astype(F32) + fin[g, 0].astype(F32) + fin[g, 1].astype(F32)).astype(BF16)
        back[g] = pack(total)
        for i in range(BLOCKS):
            if g == 0 and i == 0:
                pltpu.make_async_copy(back.at[0, 0], ret.at[0, 0], r_recv.at[0]).start()
            else:
                rcopy(back.at[g, i], ret.at[g, i], b_send.at[0], r_recv.at[g], from_offset(g * BLOCKS + i)).start()

    ta = q_ref.shape[1]
    span = NY * NC * ta

    def attend_plane(t, masked):
        kc = kbuf[t].reshape(span, kbuf.shape[-1])
        vc = jnp.concatenate([vbuf[t].reshape(span, vbuf.shape[-1]), jnp.ones((span, 128), BF16)], axis=1)
        for r in range(2 * heads):
            s = lax.dot_general(q_ref[r], kc, (((1,), (1,)), ((), ())), preferred_element_type=F32)
            if masked:
                kpos = t * span + lax.broadcasted_iota(jnp.int32, s.shape, 1)
                qpos = me * ta + lax.broadcasted_iota(jnp.int32, s.shape, 0)
                s = jnp.where(kpos <= qpos, s, NEG_LARGE)
            old = m_ref[r][:, :1]
            new = jnp.maximum(old, jnp.max(s, axis=1, keepdims=True))
            p = jnp.exp(s - new)
            scale = jnp.exp(old - new)
            m_ref[r] = jnp.broadcast_to(new, m_ref.shape[1:])
            acc_ref[r] = acc_ref[r] * scale + jnp.dot(p.astype(BF16), vc, preferred_element_type=F32)

    def attend_some(first, end):
        def step(t, carry):
            attend_plane(t, False)
            return carry

        lax.fori_loop(first, jnp.maximum(first, jnp.minimum(end, z)), step, 0)

    def attend_last():
        attend_plane(z, True)
        for h in range(heads):
            one, two = acc_ref[h], acc_ref[heads + h]
            blended = one[:, :128] / one[:, 128:] - mix_ref[h] * (two[:, :128] / two[:, 128:])
            normed = (
                blended * lax.rsqrt(jnp.mean(blended * blended, axis=1, keepdims=True) + 1e-05) * gain_ref[...]
            ).astype(BF16)
            att_ref[:, :, h * 128 : (h + 1) * 128] = normed.reshape(NX, ta // NX, 128)
        weights[3].wait()
        for r in range(NX):
            j = lax.rem(x + r, NX)
            ap[r] = jnp.dot(att_ref[j], ow_ref[...], preferred_element_type=F32).astype(BF16)
        start(attend_copies(0))

    side = ow_ref.shape[1] // 2
    one, two = pl.ds(0, side), pl.ds(side, side)

    def attend_copies(n):
        if n == 0:
            return [
                rcopy(ap.at[2, :, one], ao.at[0], at_send.at[0], at_recv.at[0], right),
                rcopy(ap.at[2, :, two], ao.at[1], at_send.at[1], at_recv.at[1], left),
                rcopy(ap.at[1, :, two], ar.at[0, :, two], at_send.at[2], at_recv.at[2], right),
                rcopy(ap.at[3, :, one], ar.at[1, :, one], at_send.at[3], at_recv.at[3], left),
            ]
        return [
            rcopy(ap.at[1, :, one], ar.at[0, :, one], at_send.at[4], at_recv.at[4], right),
            rcopy(ap.at[3, :, two], ar.at[1, :, two], at_send.at[5], at_recv.at[5], left),
        ]

    def attend_second():
        landed(attend_copies(0)[:2])
        ap[1, :, :side] = (ap[1, :, :side].astype(F32) + ao[0].astype(F32)).astype(BF16)
        ap[3, :, side:] = (ap[3, :, side:].astype(F32) + ao[1].astype(F32)).astype(BF16)
        start(attend_copies(1))

    def run(*steps):
        for step, *args in steps:
            with jax.named_scope(step.__name__ + "#" + "_".join(str(v) for v in args)):
                step(*args)

    def kv_1():
        landed(z_copies(1))
        start(z_copies(2))
        start(y_copies(1))

    def kv_2():
        landed(z_copies(2))
        start(z_copies(3))
        start(y_copies(2))
        landed(y_copies(0))
        start(hop_copies(0))

    def kv_3():
        landed(z_copies(3))
        start(z_copies(4))
        start(y_copies(3))
        landed(y_copies(1))
        start(hop_copies(1))

    def kv_4():
        landed(z_copies(4))
        start(y_copies(4))
        landed(y_copies(2))
        start(hop_copies(2))

    def kv_5():
        for k in (3, 4):
            landed(y_copies(k))
            start(hop_copies(k))

    def kv_6():
        for k in range(5):
            landed(hop_copies(k))
        start(core_copies())

    send_rows(0)
    start(z_copies(1))
    start(y_copies(0))
    for g in range(1, CHUNKS):
        send_rows(g)
    heads = q_in.shape[1]
    map_lane = lax.broadcasted_iota(jnp.int32, (q_in.shape[0], 128), 1) < 64
    with jax.named_scope("q_prep"):
        for h in range(heads):
            scaled = q_in[:, h, :].astype(F32) * 0.125
            q_ref[h] = jnp.where(map_lane, scaled, 0.0).astype(BF16)
            q_ref[heads + h] = jnp.where(map_lane, 0.0, scaled).astype(BF16)
    run((gather_first, 0), (gather_first, 1), (kv_1,), (gather_second, 0), (gather_first, 2), (kv_2,), (gather_second, 1))

    def first_half(s, carry):
        with jax.named_scope("experts"):
            experts(s)

        @pl.when(s == 0)
        def _():
            run((gather_first, 3), (kv_3,), (gather_second, 2))

        @pl.when(s == 1)
        def _():
            run((kv_4,), (gather_second, 3))

        @pl.when(s == 2)
        def _():
            run((sum_first, 2), (kv_5,))

        return carry

    lax.fori_loop(0, CHUNKS, first_half, 0)
    run((sum_first, 3), (kv_6,), (sum_second, 2), (sum_first, 1))
    with jax.named_scope("wait_kv"):
        landed(core_copies())
    m_ref[...] = jnp.full(m_ref.shape, NEG_LARGE, F32)
    acc_ref[...] = jnp.zeros(acc_ref.shape, F32)

    def second_half(s, carry):
        @pl.when(s < z)
        def _():
            with jax.named_scope("attend"):
                attend_plane(s, False)

        @pl.when(s == 1)
        def _():
            run((sum_second, 3), (sum_last, 2), (sum_first, 0))

        @pl.when(s == 4)
        def _():
            run((sum_second, 1), (sum_last, 3))

        return carry

    lax.fori_loop(0, NZ - 1, second_half, 0)
    run((attend_last,), (sum_second, 0), (sum_last, 1), (attend_second,), (sum_last, 0))

    with jax.named_scope("wait_attn"):
        landed(attend_copies(0)[2:] + attend_copies(1))
    attn_o[...] = (ap[0].astype(F32) + ar[0].astype(F32) + ar[1].astype(F32)).astype(BF16)

    for g in range(CHUNKS):
        for copy in (
            rcopy(xb.at[g, 0], xb.at[g, 1], x_send.at[0, g], x_recv.at[0, g], right),
            rcopy(xb.at[g, 0], xb.at[g, 2], x_send.at[1, g], x_recv.at[1, g], left),
            rcopy(xb.at[g, 1, top], xb.at[g, 3, top], f_send.at[0, g], f_recv.at[0, g], right),
            rcopy(xb.at[g, 2, low], xb.at[g, 3, low], f_send.at[1, g], f_recv.at[1, g], left),
            rcopy(part.at[g, 3, top], opp.at[g, 0], s1_send.at[0, g], s1_recv.at[0, g], right),
            rcopy(part.at[g, 3, low], opp.at[g, 1], s1_send.at[1, g], s1_recv.at[1, g], left),
            rcopy(part.at[g, 2, low], fin.at[g, 0, low], s2_send.at[0, g], fin_recv.at[0, g], right),
            rcopy(part.at[g, 1, top], fin.at[g, 1, top], s2_send.at[1, g], fin_recv.at[1, g], left),
            rcopy(part.at[g, 2, top], fin.at[g, 0, top], s2_send.at[2, g], fin_recv.at[2, g], right),
            rcopy(part.at[g, 1, low], fin.at[g, 1, low], s2_send.at[3, g], fin_recv.at[3, g], left),
        ):
            copy.wait_send()
    for copy in attend_copies(0) + attend_copies(1):
        copy.wait_send()
    for k in range(1, 5):
        for copy in z_copies(k):
            copy.wait_send()
    for k in range(5):
        for copy in y_copies(k) + hop_copies(k):
            copy.wait_send()
    for copy in core_copies():
        copy.wait_send()
    for sem, buf in ((a_send, outbound), (b_send, back)):
        for g in range(CHUNKS):
            blocks = buf.at[g, pl.ds(1, BLOCKS - 1)] if g == 0 else buf.at[g]
            rcopy(blocks, blocks, sem.at[0], r_recv.at[g], right).wait_send()

    def collect(n, carry):
        g = jnp.where(n < 2, n + 2, 3 - n)
        with jax.named_scope("wait_ret"):
            pltpu.make_async_copy(ret.at[g], ret.at[g], r_recv.at[g]).wait()

        def store(kq, value):
            rows_ref[pl.ds(pl.multiple_of(g * GROUP, GROUP), GROUP), kq * width : (kq + 1) * width] = value

        relayout_in(ret, g, store)
        return carry

    lax.fori_loop(0, CHUNKS, collect, 0)
    tokens = tok
    for kq in range(QUARTERS):
        both = jnp.dot(comb_ref[...], rows_ref[:, kq * width : (kq + 1) * width], preferred_element_type=F32)
        moe_o[:, kq * width : (kq + 1) * width] = (both[:tokens] + both[tokens:]).astype(BF16)


def settle(attn_in, moe_in, attn_o, moe_o):
    attn_o[...] = attn_in[...]
    moe_o[...] = moe_in[...]


def body(
    queries,
    keys,
    values,
    mix_scale,
    head_gain,
    out_weight,
    moe_input,
    norm_gain,
    routes,
    route_weights,
    gate_weight,
    up_weight,
    down_weight,
):
    ta, heads, qd = queries.shape
    tok, model = moe_input.shape
    ffe = gate_weight.shape[2]
    vd = values.shape[2]
    width = model // QUARTERS
    slots = CHUNKS * GROUP
    vmem = pl.BlockSpec(memory_space=pltpu.VMEM)
    hbm = pl.BlockSpec(memory_space=pl.ANY)
    dma = pltpu.SemaphoreType.DMA
    size = BLOCKS * QUARTERS * CAP
    attn_out, moe_out = pl.pallas_call(
        kernel,
        out_shape=(
            jax.ShapeDtypeStruct((ta // NX, model), BF16),
            jax.ShapeDtypeStruct((tok, model), BF16),
        ),
        in_specs=[vmem] * 5 + [vmem] * 2 + [pl.BlockSpec(memory_space=pltpu.SMEM), vmem] + [hbm] * 4,
        out_specs=(vmem, vmem),
        scratch_shapes=[
            pltpu.VMEM((model, ffe), BF16),
            pltpu.VMEM((model, ffe), BF16),
            pltpu.VMEM((ffe, model), BF16),
            pltpu.VMEM((heads * vd, model), BF16),
            pltpu.VMEM((CHUNKS, BLOCKS, QUARTERS * CAP, width), BF16),
            pltpu.VMEM((2 * heads, ta, qd), BF16),
            pltpu.VMEM((2 * tok, slots), BF16),
            pltpu.VMEM((NZ, NY, NC, ta, qd), BF16),
            pltpu.VMEM((NZ, NY, NC, ta, vd), BF16),
            pltpu.VMEM((size, size), BF16),
            pltpu.VMEM((size, size), BF16),
            pltpu.VMEM((CHUNKS, BLOCKS, QUARTERS * CAP, width), BF16),
            pltpu.VMEM((CHUNKS, NX, GROUP, model), BF16),
            pltpu.VMEM((NX * GROUP, ffe), BF16),
            pltpu.VMEM((CHUNKS, NX, GROUP, model), BF16),
            pltpu.VMEM((CHUNKS, 2, GROUP // 2, model), BF16),
            pltpu.VMEM((CHUNKS, 2, GROUP, model), BF16),
            pltpu.VMEM((CHUNKS, BLOCKS, QUARTERS * CAP, width), BF16),
            pltpu.VMEM((CHUNKS, BLOCKS, QUARTERS * CAP, width), BF16),
            pltpu.VMEM((slots, model), BF16),
            pltpu.VMEM((2 * heads, ta, 128), F32),
            pltpu.VMEM((2 * heads, ta, 2 * vd), F32),
            pltpu.VMEM((NX, ta // NX, heads * vd), BF16),
            pltpu.VMEM((NX, ta // NX, model), BF16),
            pltpu.VMEM((2, ta // NX, model // 2), BF16),
            pltpu.VMEM((2, ta // NX, model), BF16),
            dma((4,)),
            dma((2,)),
            dma((4, 2, 2)),
            dma((4, 2, 2)),
            dma((5, 2, 2, 2)),
            dma((5, 2, 2, 2)),
            dma((5, 2, 2)),
            dma((5, 2, 2)),
            dma((2,)),
            dma((2,)),
            dma((1,)),
            dma((CHUNKS,)),
            dma((2, CHUNKS)),
            dma((2, CHUNKS)),
            dma((2, CHUNKS)),
            dma((2, CHUNKS)),
            dma((2, CHUNKS)),
            dma((2, CHUNKS)),
            dma((4, CHUNKS)),
            dma((4, CHUNKS)),
            dma((1,)),
            dma((CHUNKS,)),
            dma((6,)),
            dma((6,)),
        ],
        compiler_params=pltpu.CompilerParams(collective_id=0, has_side_effects=True, vmem_limit_bytes=62 * 1024 * 1024),
    )(
        moe_input,
        norm_gain.reshape(1, model),
        routes.T,
        route_weights.T,
        queries,
        keys.reshape(ta, qd),
        values.reshape(ta, vd),
        mix_scale,
        head_gain.reshape(1, vd),
        out_weight.reshape(heads * vd, model),
        gate_weight[0],
        up_weight[0],
        down_weight[0],
    )
    return pl.pallas_call(
        settle,
        out_shape=(
            jax.ShapeDtypeStruct(attn_out.shape, BF16),
            jax.ShapeDtypeStruct(moe_out.shape, BF16),
        ),
        in_specs=[vmem] * 2,
        out_specs=(vmem, vmem),
    )(attn_out, moe_out)


def solution(mesh):
    split = Mesh(mesh.devices.reshape(NZ, NY, NC, NX), EP_TP)
    placed = (
        P(EP, "tp", None),
        P(EP, "tp", None),
        P(EP, "tp", None),
        P("tp"),
        P(),
        P("tp", None, None),
        P(EP_TP, None),
        P(),
        P(EP_TP, None),
        P(EP_TP, None),
        P(EP, None, "tp"),
        P(EP, None, "tp"),
        P(EP, "tp", None),
    )
    return jax.shard_map(
        body,
        mesh=split,
        in_specs=placed,
        out_specs=(P(EP_TP, None), P(EP_TP, None)),
        check_vma=False,
    )
```

```python
import functools

import jax
import jax.numpy as jnp
from jax import lax
from jax.experimental import pallas as pl
from jax.experimental.pallas import tpu as pltpu
from jax.sharding import Mesh
from jax.sharding import PartitionSpec as P

EP = ("ep_0", "ep_1", "ep_2")
EP_TP = ("ep_0", "ep_1", "ep_2", "tp")
MESH = pl.DeviceIdType.MESH

NZ, NY, NC, NX = 8, 4, 2, 4
CHUNKS = 4
BLOCKS = NZ * NY * NC // CHUNKS
CAP = 4
QUARTERS = 4
GROUP = BLOCKS * CAP
NEG_LARGE = -1e30
F32 = jnp.float32
BF16 = jnp.bfloat16


def offsets():
    out = [(0, dy, dc) for dy in range(NY) for dc in range(NC)]
    for k in (1, 2, 3):
        out += [(dz, dy, dc) for dc in range(NC) for dy in range(NY) for dz in (k, NZ - k)]
    out += [(NZ // 2, dy, dc) for dy in range(NY) for dc in range(NC)]
    return sum([out[n * BLOCKS : (n + 1) * BLOCKS] for n in (0, 2, 3, 1)], [])


OFFSETS = offsets()


def place_of(dz, dy, dc):
    k = jnp.minimum(dz, NZ - dz)
    ends = dy * NC + dc
    between = 16 * k - 8 + dc * 8 + dy * 2 + (dz > NZ // 2).astype(jnp.int32)
    place = jnp.where(k == 0, ends, jnp.where(k == NZ // 2, 56 + ends, between))
    chunk = place >> 4
    return jnp.where(chunk == 0, 0, jnp.where(chunk == 1, 3, chunk - 1)) * BLOCKS + (place & (BLOCKS - 1))


def kernel(
    tok_ref,
    ng_ref,
    routes_ref,
    rw_ref,
    q_in,
    k_ref,
    v_ref,
    mix_ref,
    gain_ref,
    ow_hbm,
    gw_hbm,
    uw_hbm,
    dw_hbm,
    attn_o,
    moe_o,
    gw,
    uw,
    dw,
    ow_ref,
    outbound,
    q_ref,
    comb_ref,
    comb_last,
    sum_ref,
    kbuf,
    vbuf,
    perm,
    perm_t,
    arr,
    xb,
    hid,
    part,
    opp,
    fin,
    back,
    ret,
    rows_ref,
    m_ref,
    acc_ref,
    att_ref,
    ap,
    ao,
    ar,
    w_sem,
    kv_own,
    z_recv,
    y_recv,
    h_recv,
    c_recv,
    a_send,
    a_recv,
    x_recv,
    f_recv,
    s1_recv,
    fin_recv,
    r_recv,
    at_recv,
):
    z = lax.axis_index("ep_0")
    y = lax.axis_index("ep_1")
    c = lax.axis_index("ep_2")
    x = lax.axis_index("tp")
    me = z * (NY * NC) + y * NC + c
    right = {"tp": lax.rem(x + 1, NX)}
    left = {"tp": lax.rem(x + NX - 1, NX)}
    y_up = {"ep_1": lax.rem(y + 1, NY)}
    y_down = {"ep_1": lax.rem(y + NY - 1, NY)}
    ym1 = lax.rem(y + NY - 1, NY)
    yp1 = lax.rem(y + 1, NY)
    partner = {"ep_2": 1 - c}

    def rcopy(src, dst, ssem, rsem, dev):
        return pltpu.make_async_remote_copy(
            src_ref=src, dst_ref=dst, send_sem=ssem, recv_sem=rsem, device_id=dev, device_id_type=MESH
        )

    barrier = pltpu.get_barrier_semaphore()

    def at_offset(i):
        dz, dy, dc = OFFSETS[i]
        return {"ep_0": lax.rem(z + dz, NZ), "ep_1": lax.rem(y + dy, NY), "ep_2": (1 - c) if dc else c}

    def from_offset(i):
        dz, dy, dc = OFFSETS[i]
        return {"ep_0": lax.rem(z + NZ - dz, NZ), "ep_1": lax.rem(y + NY - dy, NY), "ep_2": (1 - c) if dc else c}

    for i in range(CHUNKS * BLOCKS - 1, 0, -1):
        pl.semaphore_signal(barrier, inc=1, device_id=at_offset(i), device_id_type=MESH)
    for r in range(1, NX):
        pl.semaphore_signal(barrier, inc=1, device_id={"tp": lax.rem(x + r, NX)}, device_id_type=MESH)

    kv = ((k_ref, kbuf, 0), (v_ref, vbuf, 1))
    for ref, buf, j in kv:
        pltpu.make_async_copy(ref, buf.at[z, y, c], kv_own.at[j]).start()
    weights = [
        pltpu.make_async_copy(s, d, w_sem.at[i])
        for i, (s, d) in enumerate(((gw_hbm, gw), (uw_hbm, uw), (dw_hbm, dw), (ow_hbm, ow_ref)))
    ]
    for copy in weights:
        copy.start()

    size = BLOCKS * QUARTERS * CAP
    r_io = lax.broadcasted_iota(jnp.int32, (size, size), 0)
    c_io = lax.broadcasted_iota(jnp.int32, (size, size), 1)

    def packed_place(r):
        return (r % GROUP) // CAP * (QUARTERS * CAP) + r // GROUP * CAP + r % CAP

    perm[...] = (packed_place(r_io) == c_io).astype(BF16)
    perm_t[...] = (packed_place(c_io) == r_io).astype(BF16)

    tok = tok_ref.shape[0]
    slots = CHUNKS * GROUP
    sub = lax.broadcasted_iota(jnp.int32, (tok, tok), 0)
    lane = lax.broadcasted_iota(jnp.int32, (tok, tok), 1)
    same = sub == lane

    def as_col(row, zero):
        return jnp.sum(jnp.where(same, jnp.broadcast_to(row, (tok, tok)), zero), axis=1, keepdims=True)

    named = [routes_ref[k : k + 1, :] for k in range(2)]
    cols = [as_col(row, 0) for row in named]
    slot_iota = lax.broadcasted_iota(jnp.int32, (slots, tok), 0)
    place_iota = lax.broadcasted_iota(jnp.int32, (tok, slots), 1)
    dispatch = jnp.zeros((slots, tok), F32)
    comb = jnp.zeros((tok, slots), F32)
    for k in range(2):
        e = named[k]
        rank = jnp.sum(
            jnp.where(sub < lane, (cols[0] == e).astype(jnp.int32) + (cols[1] == e).astype(jnp.int32), 0),
            axis=0,
            keepdims=True,
        )
        ez, ey, ec = e >> 3, (e >> 1) & (NY - 1), e & (NC - 1)
        offset = place_of((ez + NZ - z) & (NZ - 1), (ey + NY - y) & (NY - 1), (ec + c) & (NC - 1))
        slot = offset * CAP + rank
        dispatch = dispatch + (slot_iota == slot).astype(F32)
        comb = comb + jnp.where(place_iota == as_col(slot, 0), as_col(rw_ref[k : k + 1, :], 0.0), 0.0)
    high = comb.astype(BF16)
    both = jnp.concatenate([high, (comb - high.astype(F32)).astype(BF16)], axis=0)
    comb_ref[...] = both[:, : slots - GROUP]
    comb_last[...] = both[:, slots - GROUP :]
    widened = tok_ref[...].astype(F32)
    normed = (
        widened * lax.rsqrt(jnp.mean(widened * widened, axis=1, keepdims=True) + 1e-06) * ng_ref[...]
    ).astype(BF16)
    ordered = jnp.dot(dispatch.astype(BF16), normed, preferred_element_type=F32).astype(BF16)
    width = ordered.shape[1] // QUARTERS

    def pack(block):
        tall = jnp.concatenate([block[:, kq * width : (kq + 1) * width] for kq in range(QUARTERS)], axis=0)
        turned = jnp.dot(perm_t[...], tall, preferred_element_type=F32).astype(BF16)
        return turned.reshape(BLOCKS, QUARTERS * CAP, width)

    for g in range(CHUNKS):
        outbound[g] = pack(ordered[g * GROUP : (g + 1) * GROUP])
    for ref, buf, j in kv:
        pltpu.make_async_copy(ref, buf.at[z, y, c], kv_own.at[j]).wait()
    with jax.named_scope("barrier"):
        pl.semaphore_wait(barrier, CHUNKS * BLOCKS - 1 + NX - 1)

    z_up = {"ep_0": lax.rem(z + 1, NZ)}
    z_down = {"ep_0": lax.rem(z + NZ - 1, NZ)}

    def zb(k):
        return lax.rem(z + NZ + k, NZ)

    def z_copies(k):
        ups = [rcopy(b.at[zb(1 - k), y, c], b.at[zb(1 - k), y, c], a_send.at[0], z_recv.at[k - 1, 0, j], z_up)
               for _, b, j in kv if k < 4 or j == 0]
        downs = [rcopy(b.at[zb(k - 1), y, c], b.at[zb(k - 1), y, c], a_send.at[0], z_recv.at[k - 1, 1, j], z_down)
                 for _, b, j in kv if k < 4 or j == 1]
        return ups + downs

    def z_blocks(k):
        return (0,) if k == 0 else (4,) if k == 4 else (-k, k)

    def y_copies(k):
        out = []
        for n, dz in enumerate(z_blocks(k)):
            for _, b, j in kv:
                ref = b.at[zb(dz), y, c]
                for d, dev in enumerate((y_up, y_down)):
                    out.append(rcopy(ref, ref, a_send.at[0], y_recv.at[k, n, d, j], dev))
        return out

    def hop_copies(k):
        out = []
        for n, dz in enumerate(z_blocks(k)):
            lo = kbuf.at[zb(dz), ym1, c]
            out.append(rcopy(lo, lo, a_send.at[0], h_recv.at[k, n, 0], y_up))
            hi = vbuf.at[zb(dz), yp1, c]
            out.append(rcopy(hi, hi, a_send.at[0], h_recv.at[k, n, 1], y_down))
        return out

    def core_copies(n):
        col = lax.rem(y + n, NY)
        return [rcopy(b.at[:, col, c], b.at[:, col, c], a_send.at[0], c_recv.at[n, j], partner) for _, b, j in kv]

    def start(copies):
        for copy in copies:
            copy.start()

    def landed(copies):
        for copy in copies:
            copy.wait_recv()

    def send_rows(g):
        for i in range(BLOCKS):
            if g == 0 and i == 0:
                pltpu.make_async_copy(outbound.at[0, 0], arr.at[0, 0], a_recv.at[0]).start()
            else:
                rcopy(outbound.at[g, i], arr.at[g, i], a_send.at[0], a_recv.at[g], at_offset(g * BLOCKS + i)).start()

    def relayout_in(src, g, store):
        tile = src[g].reshape(size, width)
        turned = jnp.dot(perm[...], tile, preferred_element_type=F32).astype(BF16)
        for kq in range(QUARTERS):
            store(kq, turned[kq * GROUP : (kq + 1) * GROUP])

    def gather_first(g):
        pltpu.make_async_copy(arr.at[g], arr.at[g], a_recv.at[g]).wait()

        def store(kq, value):
            xb[g, 0, :, kq * width : (kq + 1) * width] = value

        relayout_in(arr, g, store)
        rcopy(xb.at[g, 0], xb.at[g, 1], a_send.at[0], x_recv.at[0, g], right).start()
        rcopy(xb.at[g, 0], xb.at[g, 2], a_send.at[0], x_recv.at[1, g], left).start()

    top, low = pl.ds(0, GROUP // 2), pl.ds(GROUP // 2, GROUP // 2)

    def gather_second(g):
        rcopy(xb.at[g, 0], xb.at[g, 1], a_send.at[0], x_recv.at[0, g], right).wait_recv()
        rcopy(xb.at[g, 1, top], xb.at[g, 3, top], a_send.at[0], f_recv.at[0, g], right).start()
        rcopy(xb.at[g, 0], xb.at[g, 2], a_send.at[0], x_recv.at[1, g], left).wait_recv()
        rcopy(xb.at[g, 2, low], xb.at[g, 3, low], a_send.at[0], f_recv.at[1, g], left).start()

    ffe = gw.shape[1]
    model = gw.shape[0]
    rows = NX * GROUP

    def experts(g):
        rcopy(xb.at[g, 1, top], xb.at[g, 3, top], a_send.at[0], f_recv.at[0, g], right).wait_recv()
        rcopy(xb.at[g, 2, low], xb.at[g, 3, low], a_send.at[0], f_recv.at[1, g], left).wait_recv()

        @pl.when(g == 0)
        def _():
            for copy in weights[:3]:
                copy.wait()

        inputs = xb[g].reshape(rows, model)
        for n in range(0, ffe, 256):
            w = min(256, ffe - n)
            gate = jnp.dot(inputs, gw[:, n : n + w], preferred_element_type=F32)
            up = jnp.dot(inputs, uw[:, n : n + w], preferred_element_type=F32)
            hid[:, n : n + w] = (gate / (1.0 + jnp.exp(-gate)) * up).astype(BF16)
        hidden = hid[...]
        for n in range(0, model, 256):
            part[g, :, :, n : n + 256] = (
                jnp.dot(hidden, dw[:, n : n + 256], preferred_element_type=F32).astype(BF16).reshape(NX, GROUP, 256)
            )

    def sum_first(g):
        rcopy(part.at[g, 3, top], opp.at[g, 0], a_send.at[0], s1_recv.at[0, g], right).start()
        rcopy(part.at[g, 3, low], opp.at[g, 1], a_send.at[0], s1_recv.at[1, g], left).start()
        rcopy(part.at[g, 2, low], fin.at[g, 0, low], a_send.at[0], fin_recv.at[0, g], right).start()
        rcopy(part.at[g, 1, top], fin.at[g, 1, top], a_send.at[0], fin_recv.at[1, g], left).start()

    def sum_second(g):
        rcopy(part.at[g, 3, top], opp.at[g, 0], a_send.at[0], s1_recv.at[0, g], right).wait_recv()
        part[g, 2, : GROUP // 2] = (part[g, 2, : GROUP // 2].astype(F32) + opp[g, 0].astype(F32)).astype(BF16)
        rcopy(part.at[g, 2, top], fin.at[g, 0, top], a_send.at[0], fin_recv.at[2, g], right).start()
        rcopy(part.at[g, 3, low], opp.at[g, 1], a_send.at[0], s1_recv.at[1, g], left).wait_recv()
        part[g, 1, GROUP // 2 :] = (part[g, 1, GROUP // 2 :].astype(F32) + opp[g, 1].astype(F32)).astype(BF16)
        rcopy(part.at[g, 1, low], fin.at[g, 1, low], a_send.at[0], fin_recv.at[3, g], left).start()

    def sum_last(g):
        rcopy(part.at[g, 2, low], fin.at[g, 0, low], a_send.at[0], fin_recv.at[0, g], right).wait_recv()
        rcopy(part.at[g, 1, top], fin.at[g, 1, top], a_send.at[0], fin_recv.at[1, g], left).wait_recv()
        rcopy(part.at[g, 2, top], fin.at[g, 0, top], a_send.at[0], fin_recv.at[2, g], right).wait_recv()
        rcopy(part.at[g, 1, low], fin.at[g, 1, low], a_send.at[0], fin_recv.at[3, g], left).wait_recv()
        total = (part[g, 0].astype(F32) + fin[g, 0].astype(F32) + fin[g, 1].astype(F32)).astype(BF16)
        back[g] = pack(total)
        for i in range(BLOCKS):
            if g == 0 and i == 0:
                pltpu.make_async_copy(back.at[0, 0], ret.at[0, 0], r_recv.at[0]).start()
            else:
                rcopy(back.at[g, i], ret.at[g, i], a_send.at[0], r_recv.at[g], from_offset(g * BLOCKS + i)).start()

    ta = q_ref.shape[1]
    span = NY * NC * ta

    def attend_plane(t, masked):
        kc = kbuf[t].reshape(span, kbuf.shape[-1])
        vc = jnp.concatenate([vbuf[t].reshape(span, vbuf.shape[-1]), jnp.ones((span, 128), BF16)], axis=1)
        for r in range(2 * heads):
            s = lax.dot_general(q_ref[r], kc, (((1,), (1,)), ((), ())), preferred_element_type=F32)
            if masked:
                kpos = t * span + lax.broadcasted_iota(jnp.int32, s.shape, 1)
                qpos = me * ta + lax.broadcasted_iota(jnp.int32, s.shape, 0)
                s = jnp.where(kpos <= qpos, s, NEG_LARGE)
            old = m_ref[r][:, :1]
            new = jnp.maximum(old, jnp.max(s, axis=1, keepdims=True))
            p = jnp.exp(s - new)
            scale = jnp.exp(old - new)
            m_ref[r] = jnp.broadcast_to(new, m_ref.shape[1:])
            acc_ref[r] = acc_ref[r] * scale + jnp.dot(p.astype(BF16), vc, preferred_element_type=F32)

    def attend_some(first, end):
        def step(t, carry):
            attend_plane(t, False)
            return carry

        lax.fori_loop(first, jnp.maximum(first, jnp.minimum(end, z)), step, 0)

    def attend_last():
        attend_plane(z, True)
        for h in range(heads):
            one, two = acc_ref[h], acc_ref[heads + h]
            blended = one[:, :128] / one[:, 128:] - mix_ref[h] * (two[:, :128] / two[:, 128:])
            normed = (
                blended * lax.rsqrt(jnp.mean(blended * blended, axis=1, keepdims=True) + 1e-05) * gain_ref[...]
            ).astype(BF16)
            att_ref[:, :, h * 128 : (h + 1) * 128] = normed.reshape(NX, ta // NX, 128)
        weights[3].wait()
        for r in range(NX):
            j = lax.rem(x + r, NX)
            ap[r] = jnp.dot(att_ref[j], ow_ref[...], preferred_element_type=F32).astype(BF16)
        start(attend_copies(0))

    side = ow_ref.shape[1] // 2
    one, two = pl.ds(0, side), pl.ds(side, side)

    def attend_copies(n):
        if n == 0:
            return [
                rcopy(ap.at[2, :, one], ao.at[0], a_send.at[0], at_recv.at[0], right),
                rcopy(ap.at[2, :, two], ao.at[1], a_send.at[0], at_recv.at[1], left),
                rcopy(ap.at[1, :, two], ar.at[0, :, two], a_send.at[0], at_recv.at[2], right),
                rcopy(ap.at[3, :, one], ar.at[1, :, one], a_send.at[0], at_recv.at[3], left),
            ]
        return [
            rcopy(ap.at[1, :, one], ar.at[0, :, one], a_send.at[0], at_recv.at[4], right),
            rcopy(ap.at[3, :, two], ar.at[1, :, two], a_send.at[0], at_recv.at[5], left),
        ]

    def attend_second():
        landed(attend_copies(0)[:2])
        ap[1, :, :side] = (ap[1, :, :side].astype(F32) + ao[0].astype(F32)).astype(BF16)
        ap[3, :, side:] = (ap[3, :, side:].astype(F32) + ao[1].astype(F32)).astype(BF16)
        start(attend_copies(1))

    def run(*steps):
        for step, *args in steps:
            with jax.named_scope(step.__name__ + "#" + "_".join(str(v) for v in args)):
                step(*args)

    def kv_1():
        landed(z_copies(1))
        start(z_copies(2))
        start(y_copies(1))
        send_rows(2)

    def kv_2():
        landed(z_copies(2))
        start(z_copies(3))
        start(y_copies(2))
        send_rows(3)
        landed(y_copies(0))
        start(hop_copies(0))

    def kv_3():
        landed(z_copies(3))
        start(z_copies(4))
        start(y_copies(3))
        landed(y_copies(1))
        start(hop_copies(1))

    def kv_4():
        landed(z_copies(4))
        start(y_copies(4))
        start(core_copies(0))
        landed(y_copies(2))
        start(hop_copies(2))

    def kv_5():
        for k in (3, 4):
            landed(y_copies(k))
            start(hop_copies(k))
        start(core_copies(1))
        start(core_copies(3))

    def kv_6():
        for k in range(5):
            landed(hop_copies(k))
        start(core_copies(2))

    send_rows(0)
    start(z_copies(1))
    start(y_copies(0))
    send_rows(1)
    heads = q_in.shape[1]
    map_lane = lax.broadcasted_iota(jnp.int32, (q_in.shape[0], 128), 1) < 64
    with jax.named_scope("q_prep"):
        for h in range(heads):
            scaled = q_in[:, h, :].astype(F32) * 0.125
            q_ref[h] = jnp.where(map_lane, scaled, 0.0).astype(BF16)
            q_ref[heads + h] = jnp.where(map_lane, 0.0, scaled).astype(BF16)
    run((gather_first, 0), (kv_1,), (gather_second, 0), (gather_first, 1), (kv_2,))

    def attend_begin():
        for n in range(NY):
            landed(core_copies(n))
        m_ref[...] = jnp.full(m_ref.shape, NEG_LARGE, F32)
        acc_ref[...] = jnp.zeros(acc_ref.shape, F32)

    def first_half(s, carry):
        with jax.named_scope("experts"):
            experts(s)

        @pl.when(s == 0)
        def _():
            run((sum_first, 0), (gather_second, 1), (gather_first, 2), (kv_3,))

        @pl.when(s == 1)
        def _():
            run(
                (sum_first, 1),
                (gather_first, 3),
                (gather_second, 2),
                (kv_4,),
                (kv_5,),
                (kv_6,),
                (gather_second, 3),
                (sum_second, 0),
            )

        @pl.when(s == 2)
        def _():
            run((sum_first, 2), (sum_second, 1), (sum_last, 0))

        return carry

    lax.fori_loop(0, CHUNKS, first_half, 0)
    run(
        (sum_first, 3),
        (attend_begin,),
        (attend_some, 0, 3),
        (sum_second, 2),
        (sum_last, 1),
        (attend_some, 3, 5),
        (sum_second, 3),
        (sum_last, 2),
        (attend_some, 5, NZ),
        (sum_last, 3),
        (attend_last,),
        (attend_second,),
    )

    with jax.named_scope("wait_attn"):
        landed(attend_copies(0)[2:] + attend_copies(1))
    attn_o[...] = (ap[0].astype(F32) + ar[0].astype(F32) + ar[1].astype(F32)).astype(BF16)

    for g in range(CHUNKS):
        for copy in (
            rcopy(xb.at[g, 0], xb.at[g, 1], a_send.at[0], x_recv.at[0, g], right),
            rcopy(xb.at[g, 0], xb.at[g, 2], a_send.at[0], x_recv.at[1, g], left),
            rcopy(xb.at[g, 1, top], xb.at[g, 3, top], a_send.at[0], f_recv.at[0, g], right),
            rcopy(xb.at[g, 2, low], xb.at[g, 3, low], a_send.at[0], f_recv.at[1, g], left),
            rcopy(part.at[g, 3, top], opp.at[g, 0], a_send.at[0], s1_recv.at[0, g], right),
            rcopy(part.at[g, 3, low], opp.at[g, 1], a_send.at[0], s1_recv.at[1, g], left),
            rcopy(part.at[g, 2, low], fin.at[g, 0, low], a_send.at[0], fin_recv.at[0, g], right),
            rcopy(part.at[g, 1, top], fin.at[g, 1, top], a_send.at[0], fin_recv.at[1, g], left),
            rcopy(part.at[g, 2, top], fin.at[g, 0, top], a_send.at[0], fin_recv.at[2, g], right),
            rcopy(part.at[g, 1, low], fin.at[g, 1, low], a_send.at[0], fin_recv.at[3, g], left),
        ):
            copy.wait_send()
    for copy in attend_copies(0) + attend_copies(1):
        copy.wait_send()
    for k in range(1, 5):
        for copy in z_copies(k):
            copy.wait_send()
    for k in range(5):
        for copy in y_copies(k) + hop_copies(k):
            copy.wait_send()
    for n in range(NY):
        for copy in core_copies(n):
            copy.wait_send()
    def collect(g, carry):
        with jax.named_scope("wait_ret"):
            pltpu.make_async_copy(ret.at[g], ret.at[g], r_recv.at[g]).wait()

        def store(kq, value):
            rows_ref[pl.ds(pl.multiple_of(g * GROUP, GROUP), GROUP), kq * width : (kq + 1) * width] = value

        relayout_in(ret, g, store)
        return carry

    lax.fori_loop(0, CHUNKS - 1, collect, 0)
    early = (CHUNKS - 1) * GROUP
    for kq in range(QUARTERS):
        cut = slice(kq * width, (kq + 1) * width)
        both = jnp.dot(comb_ref[...], rows_ref[:early, cut], preferred_element_type=F32)
        sum_ref[:, cut] = both[:tok] + both[tok:]
    collect(CHUNKS - 1, 0)
    with jax.named_scope("combine"):
        for kq in range(QUARTERS):
            cut = slice(kq * width, (kq + 1) * width)
            both = jnp.dot(comb_last[...], rows_ref[early:, cut], preferred_element_type=F32)
            moe_o[:, cut] = (sum_ref[:, cut] + both[:tok] + both[tok:]).astype(BF16)

    for buf in (outbound, back):
        for g in range(CHUNKS):
            blocks = buf.at[g, pl.ds(1, BLOCKS - 1)] if g == 0 else buf.at[g]
            rcopy(blocks, blocks, a_send.at[0], r_recv.at[g], right).wait_send()


def body(
    queries,
    keys,
    values,
    mix_scale,
    head_gain,
    out_weight,
    moe_input,
    norm_gain,
    routes,
    route_weights,
    gate_weight,
    up_weight,
    down_weight,
):
    ta, heads, qd = queries.shape
    tok, model = moe_input.shape
    ffe = gate_weight.shape[2]
    vd = values.shape[2]
    width = model // QUARTERS
    slots = CHUNKS * GROUP
    vmem = pl.BlockSpec(memory_space=pltpu.VMEM)
    hbm = pl.BlockSpec(memory_space=pl.ANY)
    dma = pltpu.SemaphoreType.DMA
    size = BLOCKS * QUARTERS * CAP
    attn_out, moe_out = pl.pallas_call(
        kernel,
        out_shape=(
            pltpu.VMEM((ta // NX, model), BF16),
            pltpu.VMEM((tok, model), BF16),
        ),
        in_specs=[vmem] * 5 + [vmem] * 2 + [pl.BlockSpec(memory_space=pltpu.SMEM), vmem] + [hbm] * 4,
        out_specs=(vmem, vmem),
        scratch_shapes=[
            pltpu.VMEM((model, ffe), BF16),
            pltpu.VMEM((model, ffe), BF16),
            pltpu.VMEM((ffe, model), BF16),
            pltpu.VMEM((heads * vd, model), BF16),
            pltpu.VMEM((CHUNKS, BLOCKS, QUARTERS * CAP, width), BF16),
            pltpu.VMEM((2 * heads, ta, qd), BF16),
            pltpu.VMEM((2 * tok, slots - GROUP), BF16),
            pltpu.VMEM((2 * tok, GROUP), BF16),
            pltpu.VMEM((tok, model), F32),
            pltpu.VMEM((NZ, NY, NC, ta, qd), BF16),
            pltpu.VMEM((NZ, NY, NC, ta, vd), BF16),
            pltpu.VMEM((size, size), BF16),
            pltpu.VMEM((size, size), BF16),
            pltpu.VMEM((CHUNKS, BLOCKS, QUARTERS * CAP, width), BF16),
            pltpu.VMEM((CHUNKS, NX, GROUP, model), BF16),
            pltpu.VMEM((NX * GROUP, ffe), BF16),
            pltpu.VMEM((CHUNKS, NX, GROUP, model), BF16),
            pltpu.VMEM((CHUNKS, 2, GROUP // 2, model), BF16),
            pltpu.VMEM((CHUNKS, 2, GROUP, model), BF16),
            pltpu.VMEM((CHUNKS, BLOCKS, QUARTERS * CAP, width), BF16),
            pltpu.VMEM((CHUNKS, BLOCKS, QUARTERS * CAP, width), BF16),
            pltpu.VMEM((slots, model), BF16),
            pltpu.VMEM((2 * heads, ta, 128), F32),
            pltpu.VMEM((2 * heads, ta, 2 * vd), F32),
            pltpu.VMEM((NX, ta // NX, heads * vd), BF16),
            pltpu.VMEM((NX, ta // NX, model), BF16),
            pltpu.VMEM((2, ta // NX, model // 2), BF16),
            pltpu.VMEM((2, ta // NX, model), BF16),
            dma((4,)),
            dma((2,)),
            dma((4, 2, 2)),
            dma((5, 2, 2, 2)),
            dma((5, 2, 2)),
            dma((NY, 2)),
            dma((1,)),
            dma((CHUNKS,)),
            dma((2, CHUNKS)),
            dma((2, CHUNKS)),
            dma((2, CHUNKS)),
            dma((4, CHUNKS)),
            dma((CHUNKS,)),
            dma((6,)),
        ],
        compiler_params=pltpu.CompilerParams(collective_id=0, has_side_effects=True, vmem_limit_bytes=62 * 1024 * 1024),
    )(
        moe_input,
        norm_gain.reshape(1, model),
        routes.T,
        route_weights.T,
        queries,
        keys.reshape(ta, qd),
        values.reshape(ta, vd),
        mix_scale,
        head_gain.reshape(1, vd),
        out_weight.reshape(heads * vd, model),
        gate_weight[0],
        up_weight[0],
        down_weight[0],
    )
    return (attn_out, moe_out)


def solution(mesh):
    split = Mesh(mesh.devices.reshape(NZ, NY, NC, NX), EP_TP)
    placed = (
        P(EP, "tp", None),
        P(EP, "tp", None),
        P(EP, "tp", None),
        P("tp"),
        P(),
        P("tp", None, None),
        P(EP_TP, None),
        P(),
        P(EP_TP, None),
        P(EP_TP, None),
        P(EP, None, "tp"),
        P(EP, None, "tp"),
        P(EP, "tp", None),
    )
    return jax.shard_map(
        body,
        mesh=split,
        in_specs=placed,
        out_specs=(P(EP_TP, None), P(EP_TP, None)),
        check_vma=False,
    )
```
